32 devices in a mesh: sp: 8 (over z, y), tp: 4 (over x, core).
Axes of the slice: x: 2, y: 2, z: 4, core: 2. Of those that a mesh axis runs over, the one named last changes fastest.
Arguments:
- tokens: bfloat16 [4096, 2048], P('sp', 'tp'), may hold values from -64 to 64
- conv_input: bfloat16 [2048, 1024], P(None, 'tp'), may hold values from -0.125 to 0.125
- conv_inner: bfloat16 [2048, 1024], P(None, 'tp'), may hold values from -0.125 to 0.125
- conv_outer: bfloat16 [2048, 1024], P(None, 'tp'), may hold values from -0.125 to 0.125
- conv_gate: bfloat16 [2048, 1024], P(None, 'tp'), may hold values from -0.125 to 0.125
- conv_taps: bfloat16 [3, 1024], P(None, 'tp'), may hold values from -3.5 to 3.5
- query_proj: bfloat16 [2048, 1536], P(None, 'tp'), may hold values from -8 to 8
- latent_proj: bfloat16 [2048, 256], replicated, may hold values from -1 to 1
- rope_proj: bfloat16 [2048, 32], replicated, may hold values from -0.125 to 0.125
- latent_gain: float32 [256], replicated, may hold values from 0.1 to 1.9
- key_up: bfloat16 [256, 1024], P(None, 'tp'), may hold values from -2 to 2
- value_up: bfloat16 [256, 1024], P(None, 'tp'), may hold values from -0.375 to 0.375
- attn_gate: bfloat16 [2048, 1024], P(None, 'tp'), may hold values from -0.125 to 0.125
- conv_down: bfloat16 [1024, 2048], P('tp'), may hold values from -0.1875 to 0.1875
- attn_down: bfloat16 [1024, 2048], P('tp'), may hold values from -0.75 to 0.75
Outputs:
- layer_out: bfloat16 [4096, 2048], P(('sp', 'tp'))
The draws below stay inside these ranges and needn't reach their ends.
All inputs are finite; a program needn't handle non-finite values.
Results may differ from the reference program's by a relative error of at most 0.014.
Values may be sent and summed in bfloat16 or wider, within the bound.
A program may use at most 128 MiB of HBM per device.

```python
import math
import jax
import jax.numpy as jnp
from jax import lax

D = 2048
D_CONV = 1024
HEADS = 16
NOPE = 64
ROPE = 32
VDIM = 64
KV = 256
GRID_W = 64
SEQ = 4096
N_TP = 4


def weight_pair(key):
    down_part = jnp.clip(jax.random.normal(jax.random.fold_in(key, 101), (D, KV), jnp.float32), -6.0, 6.0) * D ** (-0.5)
    up_part = jnp.clip(jax.random.normal(jax.random.fold_in(key, 102), (KV, HEADS * NOPE), jnp.float32), -6.0, 6.0) * KV ** (-0.5)
    return (down_part, up_part)


def draw_latent_proj(key, part):
    return jnp.clip(weight_pair(key)[0], -1.0, 1.0).astype(jnp.bfloat16)


def draw_key_up(key, part):
    return jnp.clip(weight_pair(key)[1], -2.0, 2.0).astype(jnp.bfloat16)


def draw_tokens(key, part):
    column = jnp.arange(D, dtype=jnp.float32) / max(D - 1, 1)
    col_noise = jax.random.uniform(jax.random.fold_in(key, 201), (D,), jnp.float32)
    row_exp = jax.random.uniform(jax.random.fold_in(key, 202), (SEQ,), jnp.float32, -0.5, 0.5)
    base_draw = jnp.clip(jax.random.normal(jax.random.fold_in(key, 204), (SEQ, D), jnp.float32), -6.0, 6.0)
    col_exp = 0.5 * column + 0.5 * col_noise - 0.5
    scaling = (10.0 ** row_exp)[:, None] * (10.0 ** col_exp)[None, :]
    values = base_draw * scaling
    return jnp.clip(values, -64.0, 64.0).astype(jnp.bfloat16)


def draw_query_proj(key, part):
    spread = (6.0 / D) ** 0.5
    whole_draw = jnp.clip(jax.random.normal(jax.random.fold_in(key, 303), (D, HEADS, NOPE + ROPE), jnp.float32), -6.0, 6.0) * spread
    return jnp.clip(whole_draw, -8.0, 8.0).reshape(D, HEADS * (NOPE + ROPE)).astype(jnp.bfloat16)


def block_levels(rng, shape, cuts, low, high):
    gain = 1.0
    for axis_at, shards_of in cuts:
        draws = jax.random.uniform(jax.random.fold_in(jax.random.fold_in(rng, 6), axis_at), (shards_of,), jnp.float32, low / len(cuts), high / len(cuts))
        gain = gain * jnp.repeat(jnp.exp(draws), shape[axis_at] // shards_of).reshape((-1,) + (1,) * (len(shape) - 1 - axis_at))
    return gain


def bell_draw(key, shape, width, bound, split=(), kind=jnp.bfloat16):
    array = width * jax.random.normal(key, shape, jnp.float32)
    if split:
        array = array * block_levels(key, shape, split, -0.22, 0.18)
    return jnp.clip(array, -bound, bound).astype(kind)


def setup_inputs(seed: int = 0) -> dict:
    splits = jax.random.split(jax.random.key(seed), 16)
    return {
        "tokens": draw_tokens(jax.random.fold_in(splits[15], 71), 0),
        "conv_input": bell_draw(splits[1], (D, D_CONV), D ** -0.5, 0.125, ((1, 4),)),
        "conv_inner": bell_draw(splits[2], (D, D_CONV), D ** -0.5, 0.125, ((1, 4),)),
        "conv_outer": bell_draw(splits[3], (D, D_CONV), D ** -0.5, 0.125, ((1, 4),)),
        "conv_gate": bell_draw(splits[4], (D, D_CONV), D ** -0.5, 0.125, ((1, 4),)),
        "conv_taps": bell_draw(splits[5], (3, D_CONV), 3 ** -0.5, 3.5, ((1, 4),)),
        "query_proj": draw_query_proj(jax.random.fold_in(splits[15], 71), 0),
        "latent_proj": draw_latent_proj(jax.random.fold_in(splits[15], 71), 0),
        "rope_proj": bell_draw(splits[8], (D, ROPE), D ** -0.5, 0.125),
        "latent_gain": jnp.clip(1.0 + 0.18 * jax.random.normal(splits[9], (KV,), jnp.float32), 0.1, 1.9),
        "key_up": draw_key_up(jax.random.fold_in(splits[15], 71), 0),
        "value_up": bell_draw(splits[11], (KV, HEADS * VDIM), KV ** -0.5, 0.375, ((1, 4),)),
        "attn_gate": bell_draw(splits[12], (D, HEADS * VDIM), D ** -0.5, 0.125, ((1, 4),)),
        "conv_down": bell_draw(splits[13], (D_CONV, D), D_CONV ** -0.5, 0.1875, ((0, 4),)),
        "attn_down": bell_draw(splits[14], (HEADS * VDIM, D), (HEADS * VDIM // 16) ** -0.5, 0.75, ((0, 4),)),
    }


rms_eps = 1e-06
rope_theta = 10000.0

def rounded(values):
    return lax.optimization_barrier(values.astype(jnp.bfloat16))

def axial_tables(positions, rope_width, grid_width):
    quarter = rope_width // 4
    frequency = rope_theta ** (-jnp.arange(quarter, dtype=jnp.float32) * 2.0 / (rope_width // 2))
    grid_row = (positions // grid_width).astype(jnp.float32)
    grid_col = (positions % grid_width).astype(jnp.float32)
    row_angle = grid_row[:, None] * frequency[None, :]
    col_angle = grid_col[:, None] * frequency[None, :]
    return (jnp.cos(row_angle), jnp.sin(row_angle), jnp.cos(col_angle), jnp.sin(col_angle))

def turn_half(vector, cos_table, sin_table):
    half_width = vector.shape[-1] // 2
    leading = vector[..., :half_width]
    trailing = vector[..., half_width:]
    return jnp.concatenate([leading * cos_table - trailing * sin_table, trailing * cos_table + leading * sin_table], axis=-1)

def axial_turn(vector, tables):
    half_width = vector.shape[-1] // 2
    return jnp.concatenate([turn_half(vector[..., :half_width], tables[0], tables[1]), turn_half(vector[..., half_width:], tables[2], tables[3])], axis=-1)

def reference(tokens, conv_input, conv_inner, conv_outer, conv_gate, conv_taps, query_proj, latent_proj, rope_proj, latent_gain, key_up, value_up, attn_gate, conv_down, attn_down):
    seq_len = tokens.shape[0]
    widened = tokens.astype(jnp.float32)
    row_scale = lax.rsqrt(lax.optimization_barrier(jnp.mean(widened * widened, axis=1, keepdims=True)) + rms_eps)

    def project(matrix):
        return jnp.dot(tokens, matrix, preferred_element_type=jnp.float32) * row_scale
    value_in = rounded(project(conv_input)).astype(jnp.float32)
    inner_in = rounded(project(conv_inner)).astype(jnp.float32)
    outer_in = rounded(project(conv_outer)).astype(jnp.float32)
    gate_in = rounded(project(conv_gate)).astype(jnp.float32)
    conv_product = rounded(inner_in * value_in).astype(jnp.float32)
    padded = jnp.pad(conv_product, ((1, 1), (0, 0)))
    tap_weights = conv_taps.astype(jnp.float32)
    conv_mixed = padded[:-2] * tap_weights[0] + padded[1:-1] * tap_weights[1] + padded[2:] * tap_weights[2]
    conv_out = (jax.nn.silu(gate_in) * outer_in * conv_mixed).astype(jnp.bfloat16)
    positions = jnp.arange(seq_len, dtype=jnp.int32)
    tables = axial_tables(positions, ROPE, GRID_W)
    head_tables = tuple((grid_table[:, None, :] for grid_table in tables))
    queries = project(query_proj).reshape(seq_len, HEADS, NOPE + ROPE)
    query_nope = queries[..., :NOPE].astype(jnp.bfloat16)
    query_rope = axial_turn(queries[..., NOPE:], head_tables).astype(jnp.bfloat16)
    latent = project(latent_proj)
    latent = (latent * lax.rsqrt(lax.optimization_barrier(jnp.mean(latent * latent, axis=1, keepdims=True)) + rms_eps) * latent_gain).astype(jnp.bfloat16)
    key_rope = axial_turn(project(rope_proj), tables).astype(jnp.bfloat16)
    key_nope = jnp.dot(latent, key_up, preferred_element_type=jnp.float32).astype(jnp.bfloat16).reshape(seq_len, HEADS, NOPE)
    key_values = jnp.dot(latent, value_up, preferred_element_type=jnp.float32).astype(jnp.bfloat16).reshape(seq_len, HEADS, VDIM)
    gate_attn = rounded(project(attn_gate)).astype(jnp.float32)
    key_wide = key_nope.astype(jnp.float32)
    rope_wide = key_rope.astype(jnp.float32)
    value_wide = key_values.astype(jnp.float32)
    block_rows = math.gcd(seq_len, 256)
    score_scale = (NOPE + ROPE) ** (-0.5)

    def attend_block(block_pair):
        nope_block, rope_block = block_pair
        scores = jnp.einsum('qhd,khd->hqk', nope_block.astype(jnp.float32), key_wide)
        scores = (scores + jnp.einsum('qhd,kd->hqk', rope_block.astype(jnp.float32), rope_wide)) * score_scale
        row_top = lax.optimization_barrier(jnp.max(scores, axis=2, keepdims=True))
        weights = jnp.exp(scores - row_top)
        weight_total = lax.optimization_barrier(jnp.sum(weights, axis=2))
        narrow = rounded(weights).astype(jnp.float32)
        attended = jnp.einsum('hqk,khd->qhd', narrow, value_wide) / weight_total.T[:, :, None]
        return attended.reshape(attended.shape[0], HEADS * VDIM)
    attended = lax.map(attend_block, (query_nope.reshape(-1, block_rows, HEADS, NOPE), query_rope.reshape(-1, block_rows, HEADS, ROPE)))
    attended = attended.reshape(seq_len, HEADS * VDIM)
    attn_out = (jax.nn.silu(gate_attn) * attended).astype(jnp.bfloat16)
    conv_width = D_CONV // N_TP
    head_width = HEADS // N_TP * VDIM
    conv_groups = conv_out.reshape(seq_len, N_TP, conv_width).transpose(1, 0, 2)
    attn_groups = attn_out.reshape(seq_len, N_TP, head_width).transpose(1, 0, 2)
    conv_blocks = conv_down.reshape(N_TP, conv_width, conv_down.shape[1])
    attn_blocks = attn_down.reshape(N_TP, head_width, attn_down.shape[1])

    def add_group(running_sum, group_terms):
        conv_part, conv_matrix, attn_part, attn_matrix = group_terms
        partial_sum = jnp.dot(conv_part, conv_matrix, preferred_element_type=jnp.float32) + jnp.dot(attn_part, attn_matrix, preferred_element_type=jnp.float32)
        return (running_sum + rounded(partial_sum).astype(jnp.float32), None)
    zeroed = jnp.zeros((seq_len, conv_down.shape[1]), jnp.float32)
    summed = lax.scan(add_group, zeroed, (conv_groups, conv_blocks, attn_groups, attn_blocks))[0]
    return summed.astype(jnp.bfloat16)
```

```python
import functools
import math

import jax
import jax.numpy as jnp
from jax import lax
from jax.experimental import pallas as pl
from jax.experimental.pallas import tpu as pltpu
from jax.sharding import PartitionSpec as P

NOPE = 64
ROPE = 32
VDIM = 64
VROWS = VDIM + 16
HW = NOPE + ROPE
GRID_W = 64
LANES = 128
EDGE = 16
rms_eps = 1e-06
rope_theta = 10000.0
MESH = pl.DeviceIdType.MESH
BF = jnp.bfloat16
F32 = jnp.float32


def silu(v):
    return v / (1.0 + jnp.exp(-v))


def dot(a, b):
    return jnp.dot(a, b, preferred_element_type=F32)


def dot_t(a, b):
    return lax.dot_general(a, b, (((1,), (1,)), ((), ())), preferred_element_type=F32)


def flip(a, s):
    out, bit = a, 1
    while bit <= s:
        if s & bit:
            out = out + bit * (1 - 2 * ((a // bit) % 2))
        bit *= 2
    return out


def body(
    dims,
    tokens, wci, wcn, wco, wcg, wq, wg, wl, wr, cd, ad, ku, vu, taps, gain,
    out,
    x_all, w_conv, w_q, w_g, w_l, w_r, w_k, w_v, v_t, w_down, kv, kn, kr, vt, qbuf, cosb, sina, sinb, tab,
    cprod, cgo, gat, halo, mix, mbuf, acc, sbuf, send_b, pbuf, xbuf, rbuf, ybuf,
    wsem, tsend, trecv, rsend, rrecv, zsend, zrecv, ysend, yrecv, msend, mrecv, hsend, hrecv,
    dsend, drecv, xsend, xrecv,
):
    n_sp, n_tp, Y, Z, R, fl, D, H, C, KV, NC, NP, KB = dims
    X = n_tp // 2
    RG = R // X
    TB = R // n_tp
    RC = R // NC
    RP = RC // 4
    A = H * VDIM
    KC = n_sp * RC
    DP = D // NP
    sp = lax.axis_index("sp")
    tp = lax.axis_index("tp")
    chip = tp // 2
    core = tp % 2
    mate = chip * 2 + (1 - core)
    zi = sp // Y
    yi = sp % Y

    loads = [
        pltpu.make_async_copy(wl, w_l, wsem.at[0]),
        pltpu.make_async_copy(wr, w_r, wsem.at[1]),
        pltpu.make_async_copy(wq, w_q, wsem.at[2]),
        pltpu.make_async_copy(wcn, w_conv.at[0], wsem.at[3]),
        pltpu.make_async_copy(wci, w_conv.at[1], wsem.at[4]),
        pltpu.make_async_copy(wco, w_conv.at[2], wsem.at[5]),
        pltpu.make_async_copy(wcg, w_conv.at[3], wsem.at[6]),
        pltpu.make_async_copy(wg, w_g, wsem.at[7]),
        pltpu.make_async_copy(ku, w_k, wsem.at[8]),
        pltpu.make_async_copy(vu, w_v, wsem.at[9]),
        pltpu.make_async_copy(cd, w_down.at[0:C, :], wsem.at[10]),
        pltpu.make_async_copy(ad, w_down.at[C:, :], wsem.at[11]),
    ]

    def cols(j):
        return pl.ds(pl.multiple_of(j * fl, fl), fl)

    own = pltpu.make_async_copy(tokens, x_all.at[:, cols(tp)], wsem.at[12])

    barrier = pltpu.get_barrier_semaphore()
    pl.semaphore_signal(barrier, inc=1, device_id={"tp": mate}, device_id_type=MESH)
    for d in range(1, X):
        peer = ((chip + d) % X) * 2 + core
        pl.semaphore_signal(barrier, inc=1, device_id={"tp": peer}, device_id_type=MESH)
    for d in range(1, n_sp):
        pl.semaphore_signal(barrier, inc=1, device_id={"sp": (sp + d) % n_sp}, device_id_type=MESH)
    own.start()
    for w in loads:
        w.start()

    lane = lax.broadcasted_iota(jnp.int32, (R, LANES), 1)
    pos = sp * R + lax.broadcasted_iota(jnp.int32, (R, LANES), 0)
    grid = jnp.where(lane < ROPE // 2, pos // GRID_W, pos % GRID_W).astype(F32)
    ang = grid * jnp.exp((lane % 8).astype(F32) * (-math.log(rope_theta) / 8.0))
    active = lane < ROPE
    first = (lane % 16) < 8
    sin = jnp.sin(ang)
    cosb[...] = jnp.where(active, jnp.cos(ang), 0.0)
    sina[...] = jnp.where(active & first, -sin, 0.0)
    sinb[...] = jnp.where(active & (~first), sin, 0.0)
    post = sp * R + lax.broadcasted_iota(jnp.int32, (8, R), 1)
    freq = jnp.exp(lax.broadcasted_iota(jnp.int32, (8, R), 0).astype(F32) * (-math.log(rope_theta) / 8.0))
    rang = (post // GRID_W).astype(F32) * freq
    cang = (post % GRID_W).astype(F32) * freq
    tab[0] = jnp.cos(rang)
    tab[1] = jnp.sin(rang)
    tab[2] = jnp.cos(cang)
    tab[3] = jnp.sin(cang)

    qbuf[...] = jnp.zeros(qbuf.shape, BF)
    ones = jnp.where(lax.broadcasted_iota(jnp.int32, (VROWS - VDIM, n_sp * R), 0) == 0, 1.0, 0.0).astype(BF)
    for h in range(H):
        vt[h, VDIM:VROWS, :] = ones
    mbuf[...] = jnp.full(mbuf.shape, -jnp.inf, F32)
    acc[...] = jnp.zeros(acc.shape, F32)

    pl.semaphore_wait(barrier, 1 + (X - 1) + (n_sp - 1))

    def send_tok(d, c):
        peer = mate if d == 0 else ((chip + d) % X) * 2 + core
        rows = pl.ds(c * RC, RC)
        return pltpu.make_async_remote_copy(
            src_ref=tokens.at[rows], dst_ref=x_all.at[rows, cols(tp)],
            send_sem=tsend.at[d, c], recv_sem=trecv.at[d, c],
            device_id={"tp": peer}, device_id_type=MESH)

    def relay_tok(d, c):
        origin = ((chip - d + X) % X) * 2 + core
        rows = pl.ds(c * RC, RC)
        part = x_all.at[rows, cols(origin)]
        return pltpu.make_async_remote_copy(
            src_ref=part, dst_ref=part,
            send_sem=rsend.at[d, c], recv_sem=rrecv.at[d, c],
            device_id={"tp": mate}, device_id_type=MESH)

    for c in range(NC):
        for d in range(1, X):
            send_tok(d, c).start()
    for c in range(NC):
        send_tok(0, c).start()

    def send_z(c, s):
        part = kv.at[c, core, yi, zi]
        return pltpu.make_async_remote_copy(
            src_ref=part, dst_ref=part, send_sem=zsend.at[c, s], recv_sem=zrecv.at[c, s],
            device_id={"sp": flip(zi, s) * Y + yi}, device_id_type=MESH)

    def send_y(c, t, s):
        part = kv.at[c, core, yi, flip(zi, s)]
        return pltpu.make_async_remote_copy(
            src_ref=part, dst_ref=part, send_sem=ysend.at[c, t, s], recv_sem=yrecv.at[c, t, s],
            device_id={"sp": zi * Y + flip(yi, t)}, device_id_type=MESH)

    def send_m(c, t, s):
        part = kv.at[c, core, flip(yi, t), flip(zi, s)]
        return pltpu.make_async_remote_copy(
            src_ref=part, dst_ref=part, send_sem=msend.at[c, t, s], recv_sem=mrecv.at[c, t, s],
            device_id={"tp": mate}, device_id_type=MESH)

    def kv_start(c):
        for s in range(1, Z):
            send_z(c, s).start()
        for t in range(1, Y):
            send_y(c, t, 0).start()
        send_m(c, 0, 0).start()

    def kv_line(c, s):
        send_z(c, s).wait_recv()
        for t in range(1, Y):
            send_y(c, t, s).start()
        send_m(c, 0, s).start()

    def kv_cross(c, s):
        for t in range(1, Y):
            send_y(c, t, s).wait_recv()
            send_m(c, t, s).start()

    def kv_done(c):
        for t in range(Y):
            for s in range(Z):
                send_m(c, t, s).wait_recv()

    def turned(v, rows):
        return (v * cosb[rows, :] + pltpu.roll(v, LANES - 8, 1) * sina[rows, :]
                + pltpu.roll(v, 8, 1) * sinb[rows, :])

    def row_scale(c):
        xf = x_all[c * RC:(c + 1) * RC, :].astype(F32)
        return lax.rsqrt(jnp.sum(xf * xf, axis=1, keepdims=True) * (1.0 / D) + rms_eps)

    def latents(c, sc):
        rows = pl.ds(c * RC, RC)
        xr = x_all[rows, :]
        lat = dot(xr, w_l[...]) * sc
        lat = lat * lax.rsqrt(jnp.mean(lat * lat, axis=1, keepdims=True) + rms_eps) * gain[...]
        rp = jnp.concatenate([dot(xr, w_r[...]) * sc, jnp.zeros((RC, LANES - ROPE), F32)], axis=1)
        rp = turned(rp, rows)
        packed = rp[0:RP]
        for g in range(1, 4):
            packed = packed + pltpu.roll(rp[g * RP:(g + 1) * RP], 32 * g, 1)
        kv[c, core, yi, zi, 0:RC, :] = jnp.where(core == 0, lat[:, 0:LANES], lat[:, LANES:]).astype(BF)
        kv[c, core, yi, zi, RC:, :] = jnp.where(core == 0, packed[0:RP // 2], packed[RP // 2:]).astype(BF)

    scale = HW ** -0.5 * math.log2(math.e)

    def queries(c, sc):
        rows = pl.ds(c * RC, RC)
        q = dot(x_all[rows, :], w_q[...]) * (sc * scale)
        width = q.shape[1]
        if width % LANES:
            q = jnp.concatenate([q, jnp.zeros((RC, LANES - width % LANES), F32)], axis=1)
        qt = q.T
        blk, off = (c * RC) // RG, (c * RC) % RG
        cr, sr, cc, sn = [tab[i, :, c * RC:(c + 1) * RC] for i in range(4)]
        for h in range(H):
            low = (h % 2) * NOPE
            at = h * HW
            a, b, e, f = [qt[at + NOPE + 8 * i:at + NOPE + 8 * (i + 1)] for i in range(4)]
            qbuf[blk, h, low:low + NOPE, off:off + RC] = qt[at:at + NOPE].astype(BF)
            qbuf[blk, h, LANES:LANES + ROPE, off:off + RC] = jnp.concatenate(
                [a * cr - b * sr, b * cr + a * sr, e * cc - f * sn, f * cc + e * sn], axis=0).astype(BF)

    def conv_in(c, sc):
        rows = pl.ds(c * RC, RC)
        xr = x_all[rows, :]
        inner = (dot(xr, w_conv[0]) * sc).astype(BF).astype(F32)
        value = (dot(xr, w_conv[1]) * sc).astype(BF).astype(F32)
        cprod[rows, :] = (inner * value).astype(BF)
        outer = (dot(xr, w_conv[2]) * sc).astype(BF).astype(F32)
        gate = (dot(xr, w_conv[3]) * sc).astype(BF).astype(F32)
        cgo[rows, :] = silu(gate) * outer

    def gate_in(c, sc):
        rows = pl.ds(c * RC, RC)
        gat[rows, :] = silu((dot(x_all[rows, :], w_g[...]) * sc).astype(BF).astype(F32))

    def send_halo(k):
        src = cprod.at[pl.ds(R - EDGE, EDGE)] if k == 0 else cprod.at[pl.ds(0, EDGE)]
        to = (sp + 1) % n_sp if k == 0 else (sp + n_sp - 1) % n_sp
        return pltpu.make_async_remote_copy(
            src_ref=src, dst_ref=halo.at[k], send_sem=hsend.at[k], recv_sem=hrecv.at[k],
            device_id={"sp": to}, device_id_type=MESH)

    def build(c):
        k0 = c * KC
        for o in range(n_sp):
            y, z = o // Z, o % Z
            r0 = k0 + o * RC
            lat = jnp.concatenate([kv[c, 0, y, z, 0:RC, :], kv[c, 1, y, z, 0:RC, :]], axis=1)
            pk = jnp.concatenate([kv[c, 0, y, z, RC:, :], kv[c, 1, y, z, RC:, :]], axis=0).astype(F32)
            kr[r0:r0 + RC, :] = jnp.concatenate(
                [pk if g == 0 else pltpu.roll(pk, LANES - 32 * g, 1) for g in range(4)], axis=0).astype(BF)
            kn[r0:r0 + RC, :] = dot(lat, w_k[...]).astype(BF)
            v = dot_t(v_t[...], lat).astype(BF)
            for h in range(H):
                vt[h, 0:VDIM, r0:r0 + RC] = v[h * VDIM:(h + 1) * VDIM]

    def attend(kq, c):
        units = [(h, j) for j in range(KC // KB) for h in range(H)]
        n = len(units)

        def score(u):
            h, j = units[u]
            rows = pl.ds(c * KC + j * KB, KB)
            p = (h // 2) * LANES
            k = jnp.concatenate([kn[rows, p:p + LANES], kr[rows, :]], axis=1)
            sbuf[u % 3] = dot(k, qbuf[kq, h])

        def top(u):
            h, _ = units[u]
            old = mbuf[kq, h]
            new = jnp.maximum(old, jnp.max(sbuf[u % 3], axis=0, keepdims=True))
            mbuf[kq, h] = new
            return new, jnp.exp2(old - new)

        def weigh(u, p, shrink):
            h, j = units[u]
            acc[kq, h] = acc[kq, h] * shrink + dot(vt[h, :, c * KC + j * KB:c * KC + (j + 1) * KB], p)

        score(0)
        if n > 1:
            score(1)
        tops = {0: top(0)}
        last = None
        for u in range(n):
            if u + 2 < n:
                score(u + 2)
            if last is not None:
                weigh(*last)
            if u + 1 < n:
                tops[u + 1] = top(u + 1)
            new, shrink = tops.pop(u)
            last = (u, jnp.exp2(sbuf[u % 3] - new).astype(BF), shrink)
        weigh(*last)

    def finish(kq):
        rows = pl.ds(pl.multiple_of(kq * RG, RG), RG)
        heads = []
        for h in range(H):
            a = acc[kq, h]
            heads.append(a[0:VDIM] / a[VDIM:VDIM + 1])
        attended = jnp.concatenate(heads, axis=0).T
        mix[rows, C:] = (gat[rows, :] * attended).astype(BF)

    def send_mate(d, i):
        return pltpu.make_async_remote_copy(
            src_ref=send_b.at[d, i], dst_ref=pbuf.at[d, i], send_sem=dsend.at[d, i], recv_sem=drecv.at[d, i],
            device_id={"tp": mate}, device_id_type=MESH)

    def send_x(d, i):
        return pltpu.make_async_remote_copy(
            src_ref=xbuf.at[d, i], dst_ref=rbuf.at[d, i], send_sem=xsend.at[d, i], recv_sem=xrecv.at[d, i],
            device_id={"tp": ((chip + d) % X) * 2 + core}, device_id_type=MESH)

    def block(kq, which, i):
        rows = pl.ds(pl.multiple_of(kq * RG + which * TB, TB), TB)
        return dot(mix[rows, :], w_down[:, i * DP:(i + 1) * DP]).astype(BF)

    def pair_sum(d, i):
        send_mate(d, i).wait_recv()
        return ybuf[i].astype(F32) + pbuf[d, i].astype(F32)

    def project_out(d):
        kq = (chip + d) % X

        def push(i):
            xbuf[d, i] = pair_sum(d, i).astype(BF)
            send_x(d, i).start()

        for i in range(NP):
            send_b[d, i] = block(kq, 1 - core, i)
            send_mate(d, i).start()
            ybuf[i] = block(kq, core, i)
            if d and i:
                push(i - 1)
        if d:
            push(NP - 1)

    def conv_out():
        send_halo(0).wait_recv()
        send_halo(1).wait_recv()
        cp = cprod[...].astype(F32)
        rid = lax.broadcasted_iota(jnp.int32, (R, C), 0)
        before = halo[0].astype(F32)[EDGE - 1:EDGE, :] * jnp.where(sp == 0, 0.0, 1.0)
        after = halo[1].astype(F32)[0:1, :] * jnp.where(sp == n_sp - 1, 0.0, 1.0)
        up = jnp.where(rid == 0, before, pltpu.roll(cp, 1, 0))
        down = jnp.where(rid == R - 1, after, pltpu.roll(cp, R - 1, 0))
        tw = taps[...].astype(F32)
        mix[:, 0:C] = (cgo[...] * (up * tw[0:1] + cp * tw[1:2] + down * tw[2:3])).astype(BF)

    near = [s for s in range(1, Z) if s < 2]
    far = [s for s in range(1, Z) if s >= 2]

    own.wait()
    loads[0].wait()
    loads[1].wait()
    for c in range(NC):
        for d in range(1, X):
            send_tok(d, c).wait_recv()
            relay_tok(d, c).start()
        send_tok(0, c).wait_recv()
        for d in range(1, X):
            relay_tok(d, c).wait_recv()
        sc = row_scale(c)
        latents(c, sc)
        kv_start(c)
        if c == 0:
            for w in loads[2:]:
                w.wait()
            v_t[...] = w_v[...].astype(F32).T.astype(BF)
        queries(c, sc)
        gate_in(c, sc)
        conv_in(c, sc)
        if c >= 2:
            for s in far:
                kv_line(c - 2, s)
            kv_cross(c - 2, 0)
        if c >= 1:
            for s in near:
                kv_line(c - 1, s)
        if c >= 3:
            for s in range(1, Z):
                kv_cross(c - 3, s)
    send_halo(0).start()
    send_halo(1).start()

    first_q = (chip + 1) % X
    last_q = chip
    for s in far:
        kv_line(NC - 2, s)
    kv_cross(NC - 2, 0)
    for s in range(1, Z):
        kv_cross(NC - 3, s)
    kv_done(0)
    build(0)
    attend(first_q, 0)
    for s in near:
        kv_line(NC - 1, s)
    kv_done(1)
    build(1)
    for s in range(1, Z):
        kv_cross(NC - 2, s)
    for s in far:
        kv_line(NC - 1, s)
    kv_cross(NC - 1, 0)
    attend(first_q, 1)
    for s in range(1, Z):
        kv_cross(NC - 1, s)
    kv_done(2)
    build(2)
    attend(first_q, 2)
    conv_out()
    kv_done(3)
    build(3)
    attend(first_q, 3)
    finish(first_q)
    for d in range(1, X):
        project_out(d)
        kq = (chip + d + 1) % X
        for c in range(NC):
            attend(kq, c)
        finish(kq)
    project_out(0)

    for i in range(NP):
        total = pair_sum(0, i)
        for d in range(1, X):
            send_x(d, i).wait_recv()
            total = total + rbuf[d, i].astype(F32)
        out[:, i * DP:(i + 1) * DP] = total.astype(BF)

    for c in range(NC):
        send_tok(0, c).wait_send()
        for d in range(1, X):
            send_tok(d, c).wait_send()
            relay_tok(d, c).wait_send()
        for s in range(Z):
            if s:
                send_z(c, s).wait_send()
            for t in range(Y):
                if t:
                    send_y(c, t, s).wait_send()
                send_m(c, t, s).wait_send()
    send_halo(0).wait_send()
    send_halo(1).wait_send()
    for i in range(NP):
        for d in range(X):
            send_mate(d, i).wait_send()
            if d:
                send_x(d, i).wait_send()


def on_device(n_sp, n_tp, tokens, wci, wcn, wco, wcg, taps, wq, wl, wr, gain, ku, vu, wg, cd, ad):
    R, fl = tokens.shape
    D, C = wci.shape
    KV = wl.shape[1]
    H = ku.shape[1] // NOPE
    A = H * VDIM
    X = n_tp // 2
    Y = X if n_sp % X == 0 else 1
    Z = n_sp // Y
    RG, TB = R // X, R // n_tp
    NC, NP = 4, 4
    RC = R // NC
    DP = D // NP
    S = n_sp * R
    KB = min(512, n_sp * RC)
    dma = pltpu.SemaphoreType.DMA
    anys = pl.BlockSpec(memory_space=pl.ANY)
    vm = pl.BlockSpec(memory_space=pltpu.VMEM)
    V = pltpu.VMEM
    return pl.pallas_call(
        functools.partial(body, (n_sp, n_tp, Y, Z, R, fl, D, H, C, KV, NC, NP, KB)),
        out_shape=jax.ShapeDtypeStruct((TB, cd.shape[1]), BF),
        in_specs=[anys] * 13 + [vm] * 2,
        out_specs=vm,
        scratch_shapes=[
            V((R, D), BF), V((4, D, C), BF), V(wq.shape, BF), V((D, A), BF),
            V((D, KV), BF), V(wr.shape, BF), V(ku.shape, BF), V(vu.shape, BF),
            V((A, KV), BF), V((C + A, cd.shape[1]), BF),
            V((NC, 2, Y, Z, RC + RC // 8, LANES), BF),
            V((S, H * NOPE), BF), V((S, LANES), BF), V((H, VROWS, S), BF), V((X, H, 2 * LANES, RG), BF),
            V((R, LANES), F32), V((R, LANES), F32), V((R, LANES), F32), V((4, 8, R), F32),
            V((R, C), BF), V((R, C), F32), V((R, A), F32), V((2, EDGE, C), BF), V((R, C + A), BF),
            V((X, H, 1, RG), F32), V((X, H, VROWS, RG), F32), V((3, KB, RG), F32),
            V((X, NP, TB, DP), BF), V((X, NP, TB, DP), BF),
            V((X, NP, TB, DP), BF), V((X, NP, TB, DP), BF), V((NP, TB, DP), BF),
            dma((13,)), dma((X, NC)), dma((X, NC)), dma((X, NC)), dma((X, NC)),
            dma((NC, Z)), dma((NC, Z)), dma((NC, Y, Z)), dma((NC, Y, Z)), dma((NC, Y, Z)), dma((NC, Y, Z)),
            dma((2,)), dma((2,)),
            dma((X, NP)), dma((X, NP)), dma((X, NP)), dma((X, NP)),
        ],
        compiler_params=pltpu.CompilerParams(
            collective_id=0, has_side_effects=True, vmem_limit_bytes=60 * 1024 * 1024),
    )(tokens, wci, wcn, wco, wcg, wq, wg, wl, wr, cd, ad, ku, vu, taps, gain.reshape(1, KV))


def solution(mesh):
    tp = P(None, "tp")
    placed = (P("sp", "tp"), tp, tp, tp, tp, tp, tp, P(), P(), P(), tp, tp, tp,
              P("tp", None), P("tp", None))
    return jax.shard_map(
        functools.partial(on_device, mesh.shape["sp"], mesh.shape["tp"]),
        mesh=mesh, in_specs=placed, out_specs=P(("sp", "tp"), None), check_vma=False)
```

```python
import functools
import math

import jax
import jax.numpy as jnp
from jax import lax
from jax.experimental import pallas as pl
from jax.experimental.pallas import tpu as pltpu
from jax.sharding import PartitionSpec as P

NOPE = 64
ROPE = 32
VDIM = 64
VROWS = VDIM + 16
HW = NOPE + ROPE
GRID_W = 64
LANES = 128
EDGE = 16
rms_eps = 1e-06
rope_theta = 10000.0
MESH = pl.DeviceIdType.MESH
BF = jnp.bfloat16
F32 = jnp.float32


def silu(v):
    return v / (1.0 + jnp.exp(-v))


def dot(a, b):
    return jnp.dot(a, b, preferred_element_type=F32)


def dot_t(a, b):
    return lax.dot_general(a, b, (((1,), (1,)), ((), ())), preferred_element_type=F32)


def flip(a, s):
    out, bit = a, 1
    while bit <= s:
        if s & bit:
            out = out + bit * (1 - 2 * ((a // bit) % 2))
        bit *= 2
    return out


def body(
    dims,
    tokens, wci, wcn, wco, wcg, wq, wg, wl, wr, cd, ad, ku, vu, taps, gain,
    out,
    x_all, w_conv, w_q, w_g, w_l, w_r, w_k, w_v, v_t, w_down, kv, kn, kr, vt, qbuf, cosb, sina, sinb, tab,
    cprod, cgo, gat, halo, mix, mbuf, acc, sbuf, send_b, pbuf, xbuf, rbuf, ybuf, obuf, zp, rpp, ssq,
    wsem, tsend, trecv, rsend, rrecv, zsend, zrecv, ysend, yrecv, msend, mrecv, hsend, hrecv,
    dsend, drecv, xsend, xrecv, osem,
):
    n_sp, n_tp, Y, Z, R, fl, D, H, C, KV, NC, NP, KB = dims
    X = n_tp // 2
    RG = R // X
    TB = R // n_tp
    RC = R // NC
    RP = RC // 4
    A = H * VDIM
    KC = n_sp * RC
    DP = D // NP
    sp = lax.axis_index("sp")
    tp = lax.axis_index("tp")
    chip = tp // 2
    core = tp % 2
    mate = chip * 2 + (1 - core)
    zi = sp // Y
    yi = sp % Y

    loads = [
        pltpu.make_async_copy(wl, w_l, wsem.at[0]),
        pltpu.make_async_copy(wr, w_r, wsem.at[1]),
        pltpu.make_async_copy(wq, w_q, wsem.at[2]),
        pltpu.make_async_copy(wcn, w_conv.at[0], wsem.at[3]),
        pltpu.make_async_copy(wci, w_conv.at[1], wsem.at[4]),
        pltpu.make_async_copy(wco, w_conv.at[2], wsem.at[5]),
        pltpu.make_async_copy(wcg, w_conv.at[3], wsem.at[6]),
        pltpu.make_async_copy(wg, w_g, wsem.at[7]),
        pltpu.make_async_copy(ku, w_k, wsem.at[8]),
        pltpu.make_async_copy(vu, w_v, wsem.at[9]),
        pltpu.make_async_copy(cd, w_down.at[0:C, :], wsem.at[10]),
        pltpu.make_async_copy(ad, w_down.at[C:, :], wsem.at[11]),
    ]

    def cols(j):
        return pl.ds(pl.multiple_of(j * fl, fl), fl)

    own = pltpu.make_async_copy(tokens, x_all.at[:, cols(tp)], wsem.at[12])

    barrier = pltpu.get_barrier_semaphore()
    pl.semaphore_signal(barrier, inc=1, device_id={"tp": mate}, device_id_type=MESH)
    for d in range(1, X):
        peer = ((chip + d) % X) * 2 + core
        pl.semaphore_signal(barrier, inc=1, device_id={"tp": peer}, device_id_type=MESH)
    for d in range(1, n_sp):
        pl.semaphore_signal(barrier, inc=1, device_id={"sp": (sp + d) % n_sp}, device_id_type=MESH)
    own.start()
    for w in loads[0:2]:
        w.start()

    lane = lax.broadcasted_iota(jnp.int32, (R, LANES), 1)
    pos = sp * R + lax.broadcasted_iota(jnp.int32, (R, LANES), 0)
    grid = jnp.where(lane < ROPE // 2, pos // GRID_W, pos % GRID_W).astype(F32)
    ang = grid * jnp.exp((lane % 8).astype(F32) * (-math.log(rope_theta) / 8.0))
    active = lane < ROPE
    first = (lane % 16) < 8
    sin = jnp.sin(ang)
    cosb[...] = jnp.where(active, jnp.cos(ang), 0.0)
    sina[...] = jnp.where(active & first, -sin, 0.0)
    sinb[...] = jnp.where(active & (~first), sin, 0.0)
    post = sp * R + lax.broadcasted_iota(jnp.int32, (8, R), 1)
    freq = jnp.exp(lax.broadcasted_iota(jnp.int32, (8, R), 0).astype(F32) * (-math.log(rope_theta) / 8.0))
    rang = (post // GRID_W).astype(F32) * freq
    cang = (post % GRID_W).astype(F32) * freq
    tab[0] = jnp.cos(rang)
    tab[1] = jnp.sin(rang)
    tab[2] = jnp.cos(cang)
    tab[3] = jnp.sin(cang)

    qbuf[...] = jnp.zeros(qbuf.shape, BF)
    ones = jnp.where(lax.broadcasted_iota(jnp.int32, (VROWS - VDIM, n_sp * R), 0) == 0, 1.0, 0.0).astype(BF)
    for h in range(H):
        vt[h, VDIM:VROWS, :] = ones
    mbuf[...] = jnp.full(mbuf.shape, -jnp.inf, F32)
    acc[...] = jnp.zeros(acc.shape, F32)

    pl.semaphore_wait(barrier, 1 + (X - 1) + (n_sp - 1))

    def send_tok(d, c):
        peer = mate if d == 0 else ((chip + d) % X) * 2 + core
        rows = pl.ds(c * RC, RC)
        return pltpu.make_async_remote_copy(
            src_ref=x_all.at[rows, cols(tp)], dst_ref=x_all.at[rows, cols(tp)],
            send_sem=tsend.at[d], recv_sem=trecv.at[d, c],
            device_id={"tp": peer}, device_id_type=MESH)

    def relay_tok(d, c):
        origin = ((chip - d + X) % X) * 2 + core
        rows = pl.ds(c * RC, RC)
        part = x_all.at[rows, cols(origin)]
        return pltpu.make_async_remote_copy(
            src_ref=part, dst_ref=part,
            send_sem=rsend.at[d], recv_sem=rrecv.at[d, c],
            device_id={"tp": mate}, device_id_type=MESH)

    own.wait()
    for c in range(NC):
        for d in range(1, X):
            send_tok(d, c).start()
    for c in range(NC):
        send_tok(0, c).start()
    for w in loads[2:]:
        w.start()

    def send_z(c, s):
        part = kv.at[c, core, yi, zi]
        return pltpu.make_async_remote_copy(
            src_ref=part, dst_ref=part, send_sem=zsend.at[0], recv_sem=zrecv.at[c, s],
            device_id={"sp": flip(zi, s) * Y + yi}, device_id_type=MESH)

    def send_y(c, t, s):
        part = kv.at[c, core, yi, flip(zi, s)]
        return pltpu.make_async_remote_copy(
            src_ref=part, dst_ref=part, send_sem=ysend.at[0], recv_sem=yrecv.at[c, t, s],
            device_id={"sp": zi * Y + flip(yi, t)}, device_id_type=MESH)

    def send_m(c, t, s):
        part = kv.at[c, core, flip(yi, t), flip(zi, s)]
        return pltpu.make_async_remote_copy(
            src_ref=part, dst_ref=part, send_sem=msend.at[0], recv_sem=mrecv.at[c],
            device_id={"tp": mate}, device_id_type=MESH)

    def kv_start(c):
        for s in range(1, Z):
            send_z(c, s).start()
        for t in range(1, Y):
            send_y(c, t, 0).start()
        send_m(c, 0, 0).start()

    def kv_line(c, s):
        send_z(c, s).wait_recv()
        for t in range(1, Y):
            send_y(c, t, s).start()
        send_m(c, 0, s).start()

    def kv_cross(c, s):
        for t in range(1, Y):
            send_y(c, t, s).wait_recv()
            send_m(c, t, s).start()

    def lines(c, peers):
        for s in peers:
            kv_line(c, s)

    def crosses(c, peers):
        for s in peers:
            kv_cross(c, s)

    def kv_done(c):
        part = kv.at[c, 1 - core]
        pltpu.make_async_remote_copy(
            src_ref=part, dst_ref=part, send_sem=msend.at[0], recv_sem=mrecv.at[c],
            device_id={"tp": mate}, device_id_type=MESH).wait_recv()

    def turned(v, rows):
        return (v * cosb[rows, :] + pltpu.roll(v, LANES - 8, 1) * sina[rows, :]
                + pltpu.roll(v, 8, 1) * sinb[rows, :])

    def feature_part(rows, j):
        xr = x_all[rows, cols(j)]
        xf = xr.astype(F32)
        return (dot(xr, w_l[cols(j), :]), dot_t(xr, w_r[:, cols(j)]), jnp.sum(xf * xf, axis=1, keepdims=True))

    def add_parts(parts):
        return tuple(functools.reduce(lambda u, v: u + v, p) for p in zip(*parts))

    def latents(c, parts):
        rows = pl.ds(c * RC, RC)
        lat, rope, total = add_parts([(zp[rows, :], rpp[rows, :], ssq[rows, :])] + parts)
        sc = lax.rsqrt(total * (1.0 / D) + rms_eps)
        lat = lat * sc
        lat = lat * lax.rsqrt(jnp.mean(lat * lat, axis=1, keepdims=True) + rms_eps) * gain[...]
        kv[c, core, yi, zi, 0:RC, :] = jnp.where(core == 0, lat[:, 0:LANES], lat[:, LANES:]).astype(BF)
        rp = jnp.concatenate([rope * sc, jnp.zeros((RC, LANES - ROPE), F32)], axis=1)
        rp = turned(rp, rows)
        packed = rp[0:RP]
        for g in range(1, 4):
            packed = packed + pltpu.roll(rp[g * RP:(g + 1) * RP], 32 * g, 1)
        kv[c, core, yi, zi, RC:, :] = jnp.where(core == 0, packed[0:RP // 2], packed[RP // 2:]).astype(BF)
        return sc

    scale = HW ** -0.5 * math.log2(math.e)

    def queries(c, sc):
        rows = pl.ds(c * RC, RC)
        q = dot(x_all[rows, :], w_q[...]) * (sc * scale)
        width = q.shape[1]
        if width % LANES:
            q = jnp.concatenate([q, jnp.zeros((RC, LANES - width % LANES), F32)], axis=1)
        qt = q.T
        blk, off = (c * RC) // RG, (c * RC) % RG
        cr, sr, cc, sn = [tab[i, :, c * RC:(c + 1) * RC] for i in range(4)]
        for h in range(H):
            low = (h % 2) * NOPE
            at = h * HW
            a, b, e, f = [qt[at + NOPE + 8 * i:at + NOPE + 8 * (i + 1)] for i in range(4)]
            qbuf[blk, h, low:low + NOPE, off:off + RC] = qt[at:at + NOPE].astype(BF)
            qbuf[blk, h, LANES:LANES + ROPE, off:off + RC] = jnp.concatenate(
                [a * cr - b * sr, b * cr + a * sr, e * cc - f * sn, f * cc + e * sn], axis=0).astype(BF)

    def conv_in(c, sc):
        rows = pl.ds(c * RC, RC)
        xr = x_all[rows, :]
        inner = (dot(xr, w_conv[0]) * sc).astype(BF).astype(F32)
        value = (dot(xr, w_conv[1]) * sc).astype(BF).astype(F32)
        cprod[rows, :] = (inner * value).astype(BF)
        outer = (dot(xr, w_conv[2]) * sc).astype(BF).astype(F32)
        gate = (dot(xr, w_conv[3]) * sc).astype(BF).astype(F32)
        cgo[rows, :] = silu(gate) * outer

    def gate_in(c, sc):
        rows = pl.ds(c * RC, RC)
        gat[rows, :] = silu((dot(x_all[rows, :], w_g[...]) * sc).astype(BF).astype(F32))

    def send_halo(k):
        src = cprod.at[pl.ds(R - EDGE, EDGE)] if k == 0 else cprod.at[pl.ds(0, EDGE)]
        to = (sp + 1) % n_sp if k == 0 else (sp + n_sp - 1) % n_sp
        return pltpu.make_async_remote_copy(
            src_ref=src, dst_ref=halo.at[k], send_sem=hsend.at[k], recv_sem=hrecv.at[k],
            device_id={"sp": to}, device_id_type=MESH)

    def build(c):
        k0 = c * KC
        n = max(1, KB // RC)
        for g0 in range(0, n_sp, n):
            lats = []
            for o in range(g0, g0 + n):
                y, z = o // Z, o % Z
                r0 = k0 + o * RC
                lats.append(jnp.concatenate([kv[c, 0, y, z, 0:RC, :], kv[c, 1, y, z, 0:RC, :]], axis=1))
                pk = jnp.concatenate([kv[c, 0, y, z, RC:, :], kv[c, 1, y, z, RC:, :]], axis=0).astype(F32)
                kr[r0:r0 + RC, :] = jnp.concatenate(
                    [pk if g == 0 else pltpu.roll(pk, LANES - 32 * g, 1) for g in range(4)], axis=0).astype(BF)
            lat = jnp.concatenate(lats, axis=0)
            r0 = k0 + g0 * RC
            kn[r0:r0 + n * RC, :] = dot(lat, w_k[...]).astype(BF)
            v = dot_t(v_t[...], lat).astype(BF)
            for h in range(H):
                vt[h, 0:VDIM, r0:r0 + n * RC] = v[h * VDIM:(h + 1) * VDIM]

    def attend(kq, c, part=None):
        units = [(h, j) for j in range(KC // KB) for h in range(H)]
        n = len(units)
        if part is not None:
            units = units[part * (n // 2):(part + 1) * (n // 2)]
            n = len(units)

        def score(u):
            h, j = units[u]
            rows = pl.ds(c * KC + j * KB, KB)
            p = (h // 2) * LANES
            k = jnp.concatenate([kn[rows, p:p + LANES], kr[rows, :]], axis=1)
            sbuf[u % 3] = dot(k, qbuf[kq, h])

        def top(u):
            h, _ = units[u]
            old = mbuf[kq, h]
            new = jnp.maximum(old, jnp.max(sbuf[u % 3], axis=0, keepdims=True))
            mbuf[kq, h] = new
            return new, jnp.exp2(old - new)

        def weigh(u, p, shrink):
            h, j = units[u]
            acc[kq, h] = acc[kq, h] * shrink + dot(vt[h, :, c * KC + j * KB:c * KC + (j + 1) * KB], p)

        score(0)
        if n > 1:
            score(1)
        tops = {0: top(0)}
        last = None
        for u in range(n):
            if u + 2 < n:
                score(u + 2)
            if last is not None:
                weigh(*last)
            if u + 1 < n:
                tops[u + 1] = top(u + 1)
            new, shrink = tops.pop(u)
            last = (u, jnp.exp2(sbuf[u % 3] - new).astype(BF), shrink)
        weigh(*last)

    def finish(kq):
        rows = pl.ds(pl.multiple_of(kq * RG, RG), RG)
        heads = []
        for h in range(H):
            a = acc[kq, h]
            heads.append(a[0:VDIM] / a[VDIM:VDIM + 1])
        attended = jnp.concatenate(heads, axis=0).T
        mix[rows, C:] = (gat[rows, :] * attended).astype(BF)

    def send_mate(d, i):
        return pltpu.make_async_remote_copy(
            src_ref=send_b.at[d, i], dst_ref=pbuf.at[d, i], send_sem=dsend.at[d], recv_sem=drecv.at[d, i],
            device_id={"tp": mate}, device_id_type=MESH)

    def send_x(d, i):
        return pltpu.make_async_remote_copy(
            src_ref=xbuf.at[d, i], dst_ref=rbuf.at[d, i], send_sem=xsend.at[d], recv_sem=xrecv.at[d, i],
            device_id={"tp": ((chip + d) % X) * 2 + core}, device_id_type=MESH)

    def block(kq, which, i):
        rows = pl.ds(pl.multiple_of(kq * RG + which * TB, TB), TB)
        return dot(mix[rows, :], w_down[:, i * DP:(i + 1) * DP]).astype(BF)

    def pair_sum(d, i):
        send_mate(d, i).wait_recv()
        return ybuf[i].astype(F32) + pbuf[d, i].astype(F32)

    def give(i):
        return pltpu.make_async_copy(obuf.at[i], out.at[:, i * DP:(i + 1) * DP], osem.at[i])

    def project_out(d):
        kq = (chip + d) % X

        def push(i):
            xbuf[d, i] = pair_sum(d, i).astype(BF)
            send_x(d, i).start()

        for i in range(NP):
            send_b[d, i] = block(kq, 1 - core, i)
            send_mate(d, i).start()
        for i in range(NP):
            ybuf[i] = block(kq, core, i)
            if d:
                push(i)

    def conv_out():
        send_halo(0).wait_recv()
        send_halo(1).wait_recv()
        cp = cprod[...].astype(F32)
        rid = lax.broadcasted_iota(jnp.int32, (R, C), 0)
        before = halo[0].astype(F32)[EDGE - 1:EDGE, :] * jnp.where(sp == 0, 0.0, 1.0)
        after = halo[1].astype(F32)[0:1, :] * jnp.where(sp == n_sp - 1, 0.0, 1.0)
        up = jnp.where(rid == 0, before, pltpu.roll(cp, 1, 0))
        down = jnp.where(rid == R - 1, after, pltpu.roll(cp, R - 1, 0))
        tw = taps[...].astype(F32)
        mix[:, 0:C] = (cgo[...] * (up * tw[0:1] + cp * tw[1:2] + down * tw[2:3])).astype(BF)

    near = [s for s in range(1, Z) if s < 2]
    far = [s for s in range(1, Z) if s >= 2]

    loads[0].wait()
    loads[1].wait()
    every = pl.ds(0, R)
    parts = [feature_part(every, tp)]
    for c in range(NC):
        send_tok(0, c).wait_recv()
    parts.append(feature_part(every, mate))
    zp[...], rpp[...], ssq[...] = add_parts(parts)

    scales = []
    for c in range(NC):
        rows = pl.ds(c * RC, RC)
        parts = []
        for d in range(1, X):
            send_tok(d, c).wait_recv()
            relay_tok(d, c).start()
            parts.append(feature_part(rows, ((chip - d + X) % X) * 2 + core))
        if c == 1:
            for w in loads[2:]:
                w.wait()
            v_t[...] = w_v[...].astype(F32).T.astype(BF)
        if c:
            conv_in(c - 1, scales[c - 1])
        for d in range(1, X):
            relay_tok(d, c).wait_recv()
            parts.append(feature_part(rows, ((chip - d + X) % X) * 2 + 1 - core))
        scales.append(latents(c, parts))
        kv_start(c)
        if c:
            queries(c - 1, scales[c - 1])
            gate_in(c - 1, scales[c - 1])
        if c >= 1:
            lines(c - 1, near)
        if c >= 2:
            crosses(c - 2, [0] + near)
            lines(c - 2, far)
        if c >= 3:
            crosses(c - 3, far)
    queries(NC - 1, scales[NC - 1])
    gate_in(NC - 1, scales[NC - 1])

    first_q = (chip + 1) % X
    kv_done(0)
    build(0)
    attend(first_q, 0)
    lines(3, near)
    crosses(2, [0] + near)
    lines(2, far)
    crosses(1, far)
    crosses(3, [0])
    conv_in(NC - 1, scales[NC - 1])
    send_halo(0).start()
    send_halo(1).start()
    kv_done(1)
    build(1)
    attend(first_q, 1, 0)
    crosses(3, near)
    attend(first_q, 1, 1)
    lines(3, far)
    crosses(2, far)
    conv_out()
    kv_done(2)
    build(2)
    attend(first_q, 2, 0)
    crosses(3, far)
    attend(first_q, 2, 1)
    kv_done(3)
    build(3)
    attend(first_q, 3)
    finish(first_q)
    for d in range(1, X):
        project_out(d)
        kq = (chip + d + 1) % X
        for c in range(NC):
            attend(kq, c)
        finish(kq)
    project_out(0)

    for i in range(NP):
        total = pair_sum(0, i)
        for d in range(1, X):
            send_x(d, i).wait_recv()
            total = total + rbuf[d, i].astype(F32)
        obuf[i] = total.astype(BF)
        give(i).start()

    def sent(ref, sem):
        pltpu.make_async_copy(ref, ref, sem).wait()

    for d in range(X):
        sent(x_all.at[:, cols(tp)], tsend.at[d])
        sent(send_b.at[d], dsend.at[d])
        if d:
            sent(x_all.at[:, cols(tp)], rsend.at[d])
            sent(xbuf.at[d], xsend.at[d])
    sent(kv.at[:, core, 0, pl.ds(0, Z - 1)], zsend.at[0])
    sent(kv.at[:, core, pl.ds(0, Y - 1)], ysend.at[0])
    sent(kv.at[:, core], msend.at[0])
    send_halo(0).wait_send()
    send_halo(1).wait_send()
    for i in range(NP):
        give(i).wait()
def on_device(n_sp, n_tp, tokens, wci, wcn, wco, wcg, taps, wq, wl, wr, gain, ku, vu, wg, cd, ad):
    R, fl = tokens.shape
    D, C = wci.shape
    KV = wl.shape[1]
    H = ku.shape[1] // NOPE
    A = H * VDIM
    X = n_tp // 2
    Y = X if n_sp % X == 0 else 1
    Z = n_sp // Y
    RG, TB = R // X, R // n_tp
    NC, NP = 4, 4
    RC = R // NC
    DP = D // NP
    S = n_sp * R
    KB = min(512, n_sp * RC)
    dma = pltpu.SemaphoreType.DMA
    anys = pl.BlockSpec(memory_space=pl.ANY)
    vm = pl.BlockSpec(memory_space=pltpu.VMEM)
    V = pltpu.VMEM
    return pl.pallas_call(
        functools.partial(body, (n_sp, n_tp, Y, Z, R, fl, D, H, C, KV, NC, NP, KB)),
        out_shape=jax.ShapeDtypeStruct((TB, cd.shape[1]), BF),
        in_specs=[anys] * 13 + [vm] * 2,
        out_specs=anys,
        scratch_shapes=[
            V((R, D), BF), V((4, D, C), BF), V(wq.shape, BF), V((D, A), BF),
            V((D, KV), BF), V((ROPE, D), BF), V(ku.shape, BF), V(vu.shape, BF),
            V((A, KV), BF), V((C + A, cd.shape[1]), BF),
            V((NC, 2, Y, Z, RC + RC // 8, LANES), BF),
            V((S, H * NOPE), BF), V((S, LANES), BF), V((H, VROWS, S), BF), V((X, H, 2 * LANES, RG), BF),
            V((R, LANES), F32), V((R, LANES), F32), V((R, LANES), F32), V((4, 8, R), F32),
            V((R, C), BF), V((R, C), F32), V((R, A), F32), V((2, EDGE, C), BF), V((R, C + A), BF),
            V((X, H, 1, RG), F32), V((X, H, VROWS, RG), F32), V((3, KB, RG), F32),
            V((X, NP, TB, DP), BF), V((X, NP, TB, DP), BF),
            V((X, NP, TB, DP), BF), V((X, NP, TB, DP), BF), V((NP, TB, DP), BF), V((NP, TB, DP), BF),
            V((R, KV), F32), V((R, ROPE), F32), V((R, 1), F32),
            dma((13,)), dma((X,)), dma((X, NC)), dma((X,)), dma((X, NC)),
            dma((1,)), dma((NC, Z)), dma((1,)), dma((NC, Y, Z)), dma((1,)), dma((NC,)),
            dma((2,)), dma((2,)),
            dma((X,)), dma((X, NP)), dma((X,)), dma((X, NP)), dma((NP,)),
        ],
        compiler_params=pltpu.CompilerParams(
            collective_id=0, has_side_effects=True, vmem_limit_bytes=60 * 1024 * 1024),
    )(tokens, wci, wcn, wco, wcg, wq, wg, wl, wr.T, cd, ad, ku, vu, taps, gain.reshape(1, KV))


def solution(mesh):
    tp = P(None, "tp")
    placed = (P("sp", "tp"), tp, tp, tp, tp, tp, tp, P(), P(), P(), tp, tp, tp,
              P("tp", None), P("tp", None))
    return jax.shard_map(
        functools.partial(on_device, mesh.shape["sp"], mesh.shape["tp"]),
        mesh=mesh, in_specs=placed, out_specs=P(("sp", "tp"), None), check_vma=False)
```

```python
import functools
import math

import jax
import jax.numpy as jnp
from jax import lax
from jax.experimental import pallas as pl
from jax.experimental.pallas import tpu as pltpu
from jax.sharding import PartitionSpec as P

NOPE = 64
ROPE = 32
VDIM = 64
VROWS = VDIM + 16
HW = NOPE + ROPE
GRID_W = 64
LANES = 128
EDGE = 16
rms_eps = 1e-06
rope_theta = 10000.0
MESH = pl.DeviceIdType.MESH
BF = jnp.bfloat16
F32 = jnp.float32


def silu(v):
    return v / (1.0 + jnp.exp(-v))


def dot(a, b):
    return jnp.dot(a, b, preferred_element_type=F32)


def dot_t(a, b):
    return lax.dot_general(a, b, (((1,), (1,)), ((), ())), preferred_element_type=F32)


def flip(a, s):
    out, bit = a, 1
    while bit <= s:
        if s & bit:
            out = out + bit * (1 - 2 * ((a // bit) % 2))
        bit *= 2
    return out


def body(
    dims,
    tokens, wci, wcn, wco, wcg, wq, wg, wl, wr, cd, ad, ku, vu, taps, gain,
    out,
    x_all, w_conv, w_q, w_g, w_l, w_r, w_k, w_v, v_t, w_down, kv, kn, kr, vt, qbuf, cosb, sina, sinb, tab,
    cprod, cgo, gat, halo, mix, mbuf, acc, sbuf, send_b, pbuf, xbuf, rbuf, ybuf, obuf, zp, rpp, ssq,
    wsem, tsend, trecv, rsend, rrecv, zsend, zrecv, ysend, yrecv, msend, mrecv, hsend, hrecv,
    dsend, drecv, xsend, xrecv, osem,
):
    n_sp, n_tp, Y, Z, R, fl, D, H, C, KV, NC, NP, KB = dims
    X = n_tp // 2
    RG = R // X
    TB = R // n_tp
    RC = R // NC
    RP = RC // 4
    A = H * VDIM
    KC = n_sp * RC
    DP = D // NP
    sp = lax.axis_index("sp")
    tp = lax.axis_index("tp")
    chip = tp // 2
    core = tp % 2
    mate = chip * 2 + (1 - core)
    zi = sp // Y
    yi = sp % Y

    loads = [
        pltpu.make_async_copy(wl, w_l, wsem.at[0]),
        pltpu.make_async_copy(wr, w_r, wsem.at[1]),
        pltpu.make_async_copy(wq, w_q, wsem.at[2]),
        pltpu.make_async_copy(wcn, w_conv.at[0], wsem.at[3]),
        pltpu.make_async_copy(wci, w_conv.at[1], wsem.at[4]),
        pltpu.make_async_copy(wco, w_conv.at[2], wsem.at[5]),
        pltpu.make_async_copy(wcg, w_conv.at[3], wsem.at[6]),
        pltpu.make_async_copy(wg, w_g, wsem.at[7]),
        pltpu.make_async_copy(ku, w_k, wsem.at[8]),
        pltpu.make_async_copy(vu, w_v, wsem.at[9]),
        pltpu.make_async_copy(cd, w_down.at[0:C, :], wsem.at[10]),
        pltpu.make_async_copy(ad, w_down.at[C:, :], wsem.at[11]),
    ]

    def cols(j):
        return pl.ds(pl.multiple_of(j * fl, fl), fl)

    own = pltpu.make_async_copy(tokens, x_all.at[:, cols(tp)], wsem.at[12])

    barrier = pltpu.get_barrier_semaphore()
    pl.semaphore_signal(barrier, inc=1, device_id={"tp": mate}, device_id_type=MESH)
    for d in range(1, X):
        peer = ((chip + d) % X) * 2 + core
        pl.semaphore_signal(barrier, inc=1, device_id={"tp": peer}, device_id_type=MESH)
    for d in range(1, n_sp):
        pl.semaphore_signal(barrier, inc=1, device_id={"sp": (sp + d) % n_sp}, device_id_type=MESH)
    own.start()
    for w in loads[0:2]:
        w.start()

    pl.semaphore_wait(barrier, 1 + (X - 1) + (n_sp - 1))

    BC = NC // X

    def rows_for(to, c):
        return pl.ds(pl.multiple_of((((to + 1) * BC + c) % NC) * RC, RC), RC)

    def rows_of(c):
        return rows_for(chip, c)

    def send_tok(d, c):
        to = (chip + d) % X
        peer = mate if d == 0 else to * 2 + core
        rows = rows_for(to, c)
        return pltpu.make_async_remote_copy(
            src_ref=x_all.at[rows, cols(tp)], dst_ref=x_all.at[rows, cols(tp)],
            send_sem=tsend.at[d], recv_sem=trecv.at[d, c],
            device_id={"tp": peer}, device_id_type=MESH)

    def relay_tok(d, c):
        origin = ((chip - d + X) % X) * 2 + core
        rows = rows_of(c)
        part = x_all.at[rows, cols(origin)]
        return pltpu.make_async_remote_copy(
            src_ref=part, dst_ref=part,
            send_sem=rsend.at[d], recv_sem=rrecv.at[d, c],
            device_id={"tp": mate}, device_id_type=MESH)

    own.wait()
    for c in range(NC):
        for d in range(1, X):
            send_tok(d, c).start()
    for c in range(NC):
        send_tok(0, c).start()
    for w in loads[2:]:
        w.start()

    def send_z(c, s):
        part = kv.at[c, core, yi, zi]
        return pltpu.make_async_remote_copy(
            src_ref=part, dst_ref=part, send_sem=zsend.at[0], recv_sem=zrecv.at[c, s],
            device_id={"sp": flip(zi, s) * Y + yi}, device_id_type=MESH)

    def send_y(c, t, s):
        part = kv.at[c, core, yi, flip(zi, s)]
        return pltpu.make_async_remote_copy(
            src_ref=part, dst_ref=part, send_sem=ysend.at[0], recv_sem=yrecv.at[c, t, s],
            device_id={"sp": zi * Y + flip(yi, t)}, device_id_type=MESH)

    def send_m(c, t, s):
        part = kv.at[c, core, flip(yi, t), flip(zi, s)]
        return pltpu.make_async_remote_copy(
            src_ref=part, dst_ref=part, send_sem=msend.at[0], recv_sem=mrecv.at[c, t],
            device_id={"tp": mate}, device_id_type=MESH)

    def kv_start(c):
        for s in range(1, Z):
            send_z(c, s).start()
        for t in range(1, Y):
            send_y(c, t, 0).start()
        send_m(c, 0, 0).start()

    def kv_line(c, s):
        send_z(c, s).wait_recv()
        for t in range(1, Y):
            send_y(c, t, s).start()
        send_m(c, 0, s).start()

    def kv_cross(c, s):
        for t in range(1, Y):
            send_y(c, t, s).wait_recv()
            send_m(c, t, s).start()

    def lines(c, peers):
        for s in peers:
            kv_line(c, s)

    def crosses(c, peers):
        for s in peers:
            kv_cross(c, s)

    def kv_done(c, t):
        part = kv.at[c, 1 - core, flip(yi, t)]
        pltpu.make_async_remote_copy(
            src_ref=part, dst_ref=part, send_sem=msend.at[0], recv_sem=mrecv.at[c, t],
            device_id={"tp": mate}, device_id_type=MESH).wait_recv()

    def turned(v, rows):
        return (v * cosb[rows, :] + pltpu.roll(v, LANES - 8, 1) * sina[rows, :]
                + pltpu.roll(v, 8, 1) * sinb[rows, :])

    def feature_part(rows, j):
        xr = x_all[rows, cols(j)]
        xf = xr.astype(F32)
        return (dot(xr, w_l[cols(j), :]), dot_t(xr, w_r[:, cols(j)]), jnp.sum(xf * xf, axis=1, keepdims=True))

    def add_parts(parts):
        return tuple(functools.reduce(lambda u, v: u + v, p) for p in zip(*parts))

    def latents(c, parts):
        rows = rows_of(c)
        lat, rope, total = add_parts([(zp[rows, :], rpp[rows, :], ssq[rows, :])] + parts)
        sc = lax.rsqrt(total * (1.0 / D) + rms_eps)
        lat = lat * sc
        lat = lat * lax.rsqrt(jnp.mean(lat * lat, axis=1, keepdims=True) + rms_eps) * gain[...]
        kv[c, core, yi, zi, 0:RC, :] = jnp.where(core == 0, lat[:, 0:LANES], lat[:, LANES:]).astype(BF)
        rp = jnp.concatenate([rope * sc, jnp.zeros((RC, LANES - ROPE), F32)], axis=1)
        rp = turned(rp, rows)
        packed = rp[0:RP]
        for g in range(1, 4):
            packed = packed + pltpu.roll(rp[g * RP:(g + 1) * RP], 32 * g, 1)
        kv[c, core, yi, zi, RC:, :] = jnp.where(core == 0, packed[0:RP // 2], packed[RP // 2:]).astype(BF)
        return sc

    scale = HW ** -0.5 * math.log2(math.e)

    def queries(c, sc):
        rows = rows_of(c)
        q = dot(x_all[rows, :], w_q[...]) * (sc * scale)
        width = q.shape[1]
        if width % LANES:
            q = jnp.concatenate([q, jnp.zeros((RC, LANES - width % LANES), F32)], axis=1)
        qt = q.T
        blk, off = (chip + 1 + c // BC) % X, (c % BC) * RC
        cr, sr, cc, sn = [tab[i, :, rows] for i in range(4)]
        for h in range(H):
            low = (h % 2) * NOPE
            at = h * HW
            a, b, e, f = [qt[at + NOPE + 8 * i:at + NOPE + 8 * (i + 1)] for i in range(4)]
            qbuf[blk, h, low:low + NOPE, off:off + RC] = qt[at:at + NOPE].astype(BF)
            qbuf[blk, h, LANES:LANES + ROPE, off:off + RC] = jnp.concatenate(
                [a * cr - b * sr, b * cr + a * sr, e * cc - f * sn, f * cc + e * sn], axis=0).astype(BF)

    def conv_in(c, sc):
        rows = rows_of(c)
        xr = x_all[rows, :]
        inner = (dot(xr, w_conv[0]) * sc).astype(BF).astype(F32)
        value = (dot(xr, w_conv[1]) * sc).astype(BF).astype(F32)
        cprod[rows, :] = (inner * value).astype(BF)
        outer = (dot(xr, w_conv[2]) * sc).astype(BF).astype(F32)
        gate = (dot(xr, w_conv[3]) * sc).astype(BF).astype(F32)
        cgo[rows, :] = silu(gate) * outer

    def gate_in(c, sc):
        rows = rows_of(c)
        gat[rows, :] = silu((dot(x_all[rows, :], w_g[...]) * sc).astype(BF).astype(F32))

    def send_halo(k):
        src = cprod.at[pl.ds(R - EDGE, EDGE)] if k == 0 else cprod.at[pl.ds(0, EDGE)]
        to = (sp + 1) % n_sp if k == 0 else (sp + n_sp - 1) % n_sp
        return pltpu.make_async_remote_copy(
            src_ref=src, dst_ref=halo.at[k], send_sem=hsend.at[k], recv_sem=hrecv.at[k],
            device_id={"sp": to}, device_id_type=MESH)

    def build(c, t):
        kv_done(c, t)
        y = flip(yi, t)
        n = max(1, min(KB // RC, Z))
        for g0 in range(0, Z, n):
            k0 = pl.multiple_of((c * Y + y) * (Z * RC) + g0 * RC, n * RC)
            lats, ropes = [], []
            for z in range(g0, g0 + n):
                lats.append(jnp.concatenate([kv[c, 0, y, z, 0:RC, :], kv[c, 1, y, z, 0:RC, :]], axis=1))
                pk = jnp.concatenate([kv[c, 0, y, z, RC:, :], kv[c, 1, y, z, RC:, :]], axis=0).astype(F32)
                ropes += [pk if g == 0 else pltpu.roll(pk, LANES - 32 * g, 1) for g in range(4)]
            lat = jnp.concatenate(lats, axis=0)
            rows = pl.ds(k0, n * RC)
            kr[rows, :] = jnp.concatenate(ropes, axis=0).astype(BF)
            kn[rows, :] = dot(lat, w_k[...]).astype(BF)
            v = dot_t(v_t[...], lat).astype(BF)
            for h in range(H):
                vt[h, 0:VDIM, rows] = v[h * VDIM:(h + 1) * VDIM]

    def attend(kq, blocks):
        units = [(h, k0 + j * KB) for k0, count in blocks for j in range(count // KB) for h in range(H)]
        n = len(units)

        def score(u):
            h, k0 = units[u]
            rows = pl.ds(pl.multiple_of(k0, KB), KB)
            p = (h // 2) * LANES
            k = jnp.concatenate([kn[rows, p:p + LANES], kr[rows, :]], axis=1)
            sbuf[u % 3] = dot(k, qbuf[kq, h])

        def top(u):
            h, _ = units[u]
            old = mbuf[kq, h]
            new = jnp.maximum(old, jnp.max(sbuf[u % 3], axis=0, keepdims=True))
            mbuf[kq, h] = new
            return new, jnp.exp2(old - new)

        def weigh(u, p, shrink):
            h, k0 = units[u]
            acc[kq, h] = acc[kq, h] * shrink + dot(vt[h, :, pl.ds(pl.multiple_of(k0, KB), KB)], p)

        score(0)
        if n > 1:
            score(1)
        tops = {0: top(0)}
        last = None
        for u in range(n):
            if u + 2 < n:
                score(u + 2)
            if last is not None:
                weigh(*last)
            if u + 1 < n:
                tops[u + 1] = top(u + 1)
            new, shrink = tops.pop(u)
            last = (u, jnp.exp2(sbuf[u % 3] - new).astype(BF), shrink)
        weigh(*last)

    def line(c, t):
        return ((c * Y + flip(yi, t)) * (Z * RC), Z * RC)

    def chunks(kq, a, b):
        attend(kq, [(c * KC, KC) for c in range(a, b)])

    cross = list(range(1, Y))

    def take(c, peers):
        for t in peers:
            build(c, t)

    def heed(kq, c, peers):
        if peers:
            attend(kq, [line(c, t) for t in peers])

    def finish(kq):
        rows = pl.ds(pl.multiple_of(kq * RG, RG), RG)
        heads = []
        for h in range(H):
            a = acc[kq, h]
            heads.append(a[0:VDIM] / a[VDIM:VDIM + 1])
        attended = jnp.concatenate(heads, axis=0).T
        mix[rows, C:] = (gat[rows, :] * attended).astype(BF)

    def send_mate(d, i):
        return pltpu.make_async_remote_copy(
            src_ref=send_b.at[d, i], dst_ref=pbuf.at[d, i], send_sem=dsend.at[d], recv_sem=drecv.at[d, i],
            device_id={"tp": mate}, device_id_type=MESH)

    def send_x(d, i):
        return pltpu.make_async_remote_copy(
            src_ref=xbuf.at[d, i], dst_ref=rbuf.at[d, i], send_sem=xsend.at[d], recv_sem=xrecv.at[d, i],
            device_id={"tp": ((chip + d) % X) * 2 + core}, device_id_type=MESH)

    def block(kq, which, i):
        rows = pl.ds(pl.multiple_of(kq * RG + which * TB, TB), TB)
        return dot(mix[rows, :], w_down[:, i * DP:(i + 1) * DP]).astype(BF)

    def pair_sum(d, i):
        send_mate(d, i).wait_recv()
        return ybuf[i].astype(F32) + pbuf[d, i].astype(F32)

    def give(i):
        return pltpu.make_async_copy(obuf.at[i], out.at[:, i * DP:(i + 1) * DP], osem.at[i])

    def project_out(d):
        kq = (chip + d) % X

        def push(i):
            xbuf[d, i] = pair_sum(d, i).astype(BF)
            send_x(d, i).start()

        for i in range(NP):
            send_b[d, i] = block(kq, 1 - core, i)
            send_mate(d, i).start()
        for i in range(NP):
            ybuf[i] = block(kq, core, i)
            if d:
                push(i)

    def conv_out():
        send_halo(0).wait_recv()
        send_halo(1).wait_recv()
        cp = cprod[...].astype(F32)
        rid = lax.broadcasted_iota(jnp.int32, (R, C), 0)
        before = halo[0].astype(F32)[EDGE - 1:EDGE, :] * jnp.where(sp == 0, 0.0, 1.0)
        after = halo[1].astype(F32)[0:1, :] * jnp.where(sp == n_sp - 1, 0.0, 1.0)
        up = jnp.where(rid == 0, before, pltpu.roll(cp, 1, 0))
        down = jnp.where(rid == R - 1, after, pltpu.roll(cp, R - 1, 0))
        tw = taps[...].astype(F32)
        mix[:, 0:C] = (cgo[...] * (up * tw[0:1] + cp * tw[1:2] + down * tw[2:3])).astype(BF)

    near = [s for s in range(1, Z) if s < 2]
    far = [s for s in range(1, Z) if s >= 2]

    loads[0].wait()
    loads[1].wait()
    every = pl.ds(0, R)
    parts = [feature_part(every, tp)]
    for c in range(NC):
        send_tok(0, c).wait_recv()
    parts.append(feature_part(every, mate))
    zp[...], rpp[...], ssq[...] = add_parts(parts)

    lane = lax.broadcasted_iota(jnp.int32, (R, LANES), 1)
    pos = sp * R + lax.broadcasted_iota(jnp.int32, (R, LANES), 0)
    grid = jnp.where(lane < ROPE // 2, pos // GRID_W, pos % GRID_W).astype(F32)
    ang = grid * jnp.exp((lane % 8).astype(F32) * (-math.log(rope_theta) / 8.0))
    active = lane < ROPE
    first = (lane % 16) < 8
    sin = jnp.sin(ang)
    cosb[...] = jnp.where(active, jnp.cos(ang), 0.0)
    sina[...] = jnp.where(active & first, -sin, 0.0)
    sinb[...] = jnp.where(active & (~first), sin, 0.0)
    post = sp * R + lax.broadcasted_iota(jnp.int32, (8, R), 1)
    freq = jnp.exp(lax.broadcasted_iota(jnp.int32, (8, R), 0).astype(F32) * (-math.log(rope_theta) / 8.0))
    rang = (post // GRID_W).astype(F32) * freq
    cang = (post % GRID_W).astype(F32) * freq
    tab[0] = jnp.cos(rang)
    tab[1] = jnp.sin(rang)
    tab[2] = jnp.cos(cang)
    tab[3] = jnp.sin(cang)

    qbuf[...] = jnp.zeros(qbuf.shape, BF)
    ones = jnp.where(lax.broadcasted_iota(jnp.int32, (VROWS - VDIM, n_sp * R), 0) == 0, 1.0, 0.0).astype(BF)
    for h in range(H):
        vt[h, VDIM:VROWS, :] = ones
    mbuf[...] = jnp.full(mbuf.shape, -jnp.inf, F32)
    acc[...] = jnp.zeros(acc.shape, F32)


    scales = []
    for c in range(NC):
        rows = rows_of(c)
        parts = []
        for d in range(1, X):
            send_tok(d, c).wait_recv()
            relay_tok(d, c).start()
            parts.append(feature_part(rows, ((chip - d + X) % X) * 2 + core))
        if c == 1:
            for w in loads[2:]:
                w.wait()
            v_t[...] = w_v[...].astype(F32).T.astype(BF)
        if c:
            conv_in(c - 1, scales[c - 1])
        for d in range(1, X):
            relay_tok(d, c).wait_recv()
            parts.append(feature_part(rows, ((chip - d + X) % X) * 2 + 1 - core))
        scales.append(latents(c, parts))
        kv_start(c)
        if c and c - 1 < BC:
            queries(c - 1, scales[c - 1])
        if c >= 1:
            lines(c - 1, near)
        if c >= 2:
            lines(c - 2, far)
        if c and c - 1 < BC:
            gate_in(c - 1, scales[c - 1])
        if c == NC - 1:
            conv_in(c, scales[c])
            send_halo(0).start()
            send_halo(1).start()
        if c >= 1:
            crosses(c - 1, [0])
        if c >= 2:
            crosses(c - 2, near)
    first_q = (chip + 1) % X
    take(0, [0])
    heed(first_q, 0, [0])
    crosses(0, far)
    lines(2, far)
    lines(3, near)
    crosses(3, [0])
    crosses(2, near)
    take(0, cross)
    take(1, [0])
    attend(first_q, [line(0, t) for t in cross] + [line(1, 0)])
    crosses(1, far)
    lines(3, far)
    take(2, [0])
    take(1, cross)
    crosses(3, near)
    crosses(2, far)
    attend(first_q, [line(1, t) for t in cross] + [line(2, 0)])
    take(3, [0])
    crosses(3, far)
    take(2, cross)
    attend(first_q, [line(2, t) for t in cross] + [line(3, 0)])
    conv_out()
    take(3, cross)
    heed(first_q, 3, cross)
    finish(first_q)
    for d in range(1, X):
        project_out(d)
        kq = (chip + d + 1) % X
        if d == 1:
            for c in range(BC, NC):
                queries(c, scales[c])
                gate_in(c, scales[c])
        for c in range(NC):
            chunks(kq, c, c + 1)
        finish(kq)
    project_out(0)

    for i in range(NP):
        total = pair_sum(0, i)
        for d in range(1, X):
            send_x(d, i).wait_recv()
            total = total + rbuf[d, i].astype(F32)
        obuf[i] = total.astype(BF)
        give(i).start()

    def sent(ref, sem):
        pltpu.make_async_copy(ref, ref, sem).wait()

    for d in range(X):
        sent(x_all.at[:, cols(tp)], tsend.at[d])
        sent(send_b.at[d], dsend.at[d])
        if d:
            sent(x_all.at[:, cols(tp)], rsend.at[d])
            sent(xbuf.at[d], xsend.at[d])
    sent(kv.at[:, core, 0, pl.ds(0, Z - 1)], zsend.at[0])
    sent(kv.at[:, core, pl.ds(0, Y - 1)], ysend.at[0])
    sent(kv.at[:, core], msend.at[0])
    send_halo(0).wait_send()
    send_halo(1).wait_send()
    for i in range(NP):
        give(i).wait()
def on_device(n_sp, n_tp, tokens, wci, wcn, wco, wcg, taps, wq, wl, wr, gain, ku, vu, wg, cd, ad):
    R, fl = tokens.shape
    D, C = wci.shape
    KV = wl.shape[1]
    H = ku.shape[1] // NOPE
    A = H * VDIM
    X = n_tp // 2
    Y = X if n_sp % X == 0 else 1
    Z = n_sp // Y
    RG, TB = R // X, R // n_tp
    NC, NP = 4, 4
    RC = R // NC
    DP = D // NP
    S = n_sp * R
    KB = min(512, n_sp * RC)
    dma = pltpu.SemaphoreType.DMA
    anys = pl.BlockSpec(memory_space=pl.ANY)
    vm = pl.BlockSpec(memory_space=pltpu.VMEM)
    V = pltpu.VMEM
    return pl.pallas_call(
        functools.partial(body, (n_sp, n_tp, Y, Z, R, fl, D, H, C, KV, NC, NP, KB)),
        out_shape=jax.ShapeDtypeStruct((TB, cd.shape[1]), BF),
        in_specs=[anys] * 13 + [vm] * 2,
        out_specs=anys,
        scratch_shapes=[
            V((R, D), BF), V((4, D, C), BF), V(wq.shape, BF), V((D, A), BF),
            V((D, KV), BF), V((ROPE, D), BF), V(ku.shape, BF), V(vu.shape, BF),
            V((A, KV), BF), V((C + A, cd.shape[1]), BF),
            V((NC, 2, Y, Z, RC + RC // 8, LANES), BF),
            V((S, H * NOPE), BF), V((S, LANES), BF), V((H, VROWS, S), BF), V((X, H, 2 * LANES, RG), BF),
            V((R, LANES), F32), V((R, LANES), F32), V((R, LANES), F32), V((4, 8, R), F32),
            V((R, C), BF), V((R, C), F32), V((R, A), F32), V((2, EDGE, C), BF), V((R, C + A), BF),
            V((X, H, 1, RG), F32), V((X, H, VROWS, RG), F32), V((3, KB, RG), F32),
            V((X, NP, TB, DP), BF), V((X, NP, TB, DP), BF),
            V((X, NP, TB, DP), BF), V((X, NP, TB, DP), BF), V((NP, TB, DP), BF), V((NP, TB, DP), BF),
            V((R, KV), F32), V((R, ROPE), F32), V((R, 1), F32),
            dma((13,)), dma((X,)), dma((X, NC)), dma((X,)), dma((X, NC)),
            dma((1,)), dma((NC, Z)), dma((1,)), dma((NC, Y, Z)), dma((1,)), dma((NC, Y)),
            dma((2,)), dma((2,)),
            dma((X,)), dma((X, NP)), dma((X,)), dma((X, NP)), dma((NP,)),
        ],
        compiler_params=pltpu.CompilerParams(
            collective_id=0, has_side_effects=True, vmem_limit_bytes=60 * 1024 * 1024),
    )(tokens, wci, wcn, wco, wcg, wq, wg, wl, wr.T, cd, ad, ku, vu, taps, gain.reshape(1, KV))


def solution(mesh):
    tp = P(None, "tp")
    placed = (P("sp", "tp"), tp, tp, tp, tp, tp, tp, P(), P(), P(), tp, tp, tp,
              P("tp", None), P("tp", None))
    return jax.shard_map(
        functools.partial(on_device, mesh.shape["sp"], mesh.shape["tp"]),
        mesh=mesh, in_specs=placed, out_specs=P(("sp", "tp"), None), check_vma=False)
```

```python
import functools
import math

import jax
import jax.numpy as jnp
from jax import lax
from jax.experimental import pallas as pl
from jax.experimental.pallas import tpu as pltpu
from jax.sharding import PartitionSpec as P

NOPE = 64
ROPE = 32
VDIM = 64
VROWS = VDIM + 16
HW = NOPE + ROPE
GRID_W = 64
LANES = 128
EDGE = 16
rms_eps = 1e-06
rope_theta = 10000.0
MESH = pl.DeviceIdType.MESH
BF = jnp.bfloat16
F32 = jnp.float32


def silu(v):
    return v / (1.0 + jnp.exp(-v))


def dot(a, b):
    return jnp.dot(a, b, preferred_element_type=F32)


def dot_t(a, b):
    return lax.dot_general(a, b, (((1,), (1,)), ((), ())), preferred_element_type=F32)


def flip(a, s):
    out, bit = a, 1
    while bit <= s:
        if s & bit:
            out = out + bit * (1 - 2 * ((a // bit) % 2))
        bit *= 2
    return out


def body(
    dims,
    tokens, wci, wcn, wco, wcg, wq, wg, wl, wr, cd, ad, ku, vu, taps, gain,
    out,
    x_all, w_conv, w_q, w_g, w_l, w_r, w_k, w_v, v_t, w_down, kv, kn, kr, vt, qbuf, cosb, sina, sinb, tab,
    cprod, cgo, gat, halo, mix, mbuf, acc, sbuf, send_b, pbuf, xbuf, rbuf, ybuf, obuf, zp, rpp, ssq,
    wsem, tsend, trecv, rsend, rrecv, zsend, zrecv, ysend, yrecv, msend, mrecv, hsend, hrecv,
    dsend, drecv, xsend, xrecv, osem,
):
    n_sp, n_tp, Y, Z, R, fl, D, H, C, KV, NC, NP, KB = dims
    X = n_tp // 2
    RG = R // X
    TB = R // n_tp
    RC = R // NC
    RP = RC // 4
    A = H * VDIM
    KC = n_sp * RC
    DP = D // NP
    sp = lax.axis_index("sp")
    tp = lax.axis_index("tp")
    chip = tp // 2
    core = tp % 2
    mate = chip * 2 + (1 - core)
    zi = sp // Y
    yi = sp % Y

    loads = [
        pltpu.make_async_copy(wl, w_l, wsem.at[0]),
        pltpu.make_async_copy(wr, w_r, wsem.at[1]),
        pltpu.make_async_copy(wq, w_q, wsem.at[2]),
        pltpu.make_async_copy(wcn, w_conv.at[0], wsem.at[3]),
        pltpu.make_async_copy(wci, w_conv.at[1], wsem.at[4]),
        pltpu.make_async_copy(wco, w_conv.at[2], wsem.at[5]),
        pltpu.make_async_copy(wcg, w_conv.at[3], wsem.at[6]),
        pltpu.make_async_copy(wg, w_g, wsem.at[7]),
        pltpu.make_async_copy(ku, w_k, wsem.at[8]),
        pltpu.make_async_copy(vu, w_v, wsem.at[9]),
        pltpu.make_async_copy(cd, w_down.at[0:C, :], wsem.at[10]),
        pltpu.make_async_copy(ad, w_down.at[C:, :], wsem.at[11]),
    ]

    def cols(j):
        return pl.ds(pl.multiple_of(j * fl, fl), fl)

    own = pltpu.make_async_copy(tokens, x_all.at[:, cols(tp)], wsem.at[12])

    barrier = pltpu.get_barrier_semaphore()
    pl.semaphore_signal(barrier, inc=1, device_id={"tp": mate}, device_id_type=MESH)
    for d in range(1, X):
        peer = ((chip + d) % X) * 2 + core
        pl.semaphore_signal(barrier, inc=1, device_id={"tp": peer}, device_id_type=MESH)
    for d in range(1, n_sp):
        pl.semaphore_signal(barrier, inc=1, device_id={"sp": (sp + d) % n_sp}, device_id_type=MESH)
    own.start()
    for w in loads[0:2]:
        w.start()

    pl.semaphore_wait(barrier, 1 + (X - 1) + (n_sp - 1))

    BC = NC // X

    def rows_for(to, c):
        return pl.ds(pl.multiple_of((((to + 1) * BC + c) % NC) * RC, RC), RC)

    def rows_of(c):
        return rows_for(chip, c)

    def send_tok(d, c):
        to = (chip + d) % X
        peer = mate if d == 0 else to * 2 + core
        rows = rows_for(to, c)
        return pltpu.make_async_remote_copy(
            src_ref=x_all.at[rows, cols(tp)], dst_ref=x_all.at[rows, cols(tp)],
            send_sem=tsend.at[d], recv_sem=trecv.at[d, c],
            device_id={"tp": peer}, device_id_type=MESH)

    def relay_tok(d, c):
        origin = ((chip - d + X) % X) * 2 + core
        rows = rows_of(c)
        part = x_all.at[rows, cols(origin)]
        return pltpu.make_async_remote_copy(
            src_ref=part, dst_ref=part,
            send_sem=rsend.at[d], recv_sem=rrecv.at[d, c],
            device_id={"tp": mate}, device_id_type=MESH)

    own.wait()
    for c in range(NC):
        for d in range(1, X):
            send_tok(d, c).start()
    for c in range(NC):
        send_tok(0, c).start()
    for w in loads[2:]:
        w.start()

    def send_z(c, s):
        part = kv.at[c, core, yi, zi]
        return pltpu.make_async_remote_copy(
            src_ref=part, dst_ref=part, send_sem=zsend.at[0], recv_sem=zrecv.at[c, s],
            device_id={"sp": flip(zi, s) * Y + yi}, device_id_type=MESH)

    def send_y(c, t, s):
        part = kv.at[c, core, yi, flip(zi, s)]
        return pltpu.make_async_remote_copy(
            src_ref=part, dst_ref=part, send_sem=ysend.at[0], recv_sem=yrecv.at[c, t, s],
            device_id={"sp": zi * Y + flip(yi, t)}, device_id_type=MESH)

    def send_m(c, t, s):
        part = kv.at[c, core, flip(yi, t), flip(zi, s)]
        return pltpu.make_async_remote_copy(
            src_ref=part, dst_ref=part, send_sem=msend.at[0], recv_sem=mrecv.at[c, t],
            device_id={"tp": mate}, device_id_type=MESH)

    def kv_start(c):
        for s in range(1, Z):
            send_z(c, s).start()
        for t in range(1, Y):
            send_y(c, t, 0).start()
        send_m(c, 0, 0).start()

    def kv_line(c, s):
        send_z(c, s).wait_recv()
        for t in range(1, Y):
            send_y(c, t, s).start()
        send_m(c, 0, s).start()

    def kv_cross(c, s):
        for t in range(1, Y):
            send_y(c, t, s).wait_recv()
            send_m(c, t, s).start()

    def lines(c, peers):
        for s in peers:
            kv_line(c, s)

    def crosses(c, peers):
        for s in peers:
            kv_cross(c, s)

    def kv_done(c, t):
        part = kv.at[c, 1 - core, flip(yi, t)]
        pltpu.make_async_remote_copy(
            src_ref=part, dst_ref=part, send_sem=msend.at[0], recv_sem=mrecv.at[c, t],
            device_id={"tp": mate}, device_id_type=MESH).wait_recv()

    def turned(v, rows):
        return (v * cosb[rows, :] + pltpu.roll(v, LANES - 8, 1) * sina[rows, :]
                + pltpu.roll(v, 8, 1) * sinb[rows, :])

    def feature_part(rows, j):
        xr = x_all[rows, cols(j)]
        xf = xr.astype(F32)
        return (dot(xr, w_l[cols(j), :]), dot_t(xr, w_r[:, cols(j)]), jnp.sum(xf * xf, axis=1, keepdims=True))

    def add_parts(parts):
        return tuple(functools.reduce(lambda u, v: u + v, p) for p in zip(*parts))

    def latents(c, parts):
        rows = rows_of(c)
        lat, rope, total = add_parts([(zp[rows, :], rpp[rows, :], ssq[rows, :])] + parts)
        sc = lax.rsqrt(total * (1.0 / D) + rms_eps)
        lat = lat * sc
        lat = lat * lax.rsqrt(jnp.mean(lat * lat, axis=1, keepdims=True) + rms_eps) * gain[...]
        kv[c, core, yi, zi, 0:RC, :] = jnp.where(core == 0, lat[:, 0:LANES], lat[:, LANES:]).astype(BF)
        rp = jnp.concatenate([rope * sc, jnp.zeros((RC, LANES - ROPE), F32)], axis=1)
        rp = turned(rp, rows)
        packed = rp[0:RP]
        for g in range(1, 4):
            packed = packed + pltpu.roll(rp[g * RP:(g + 1) * RP], 32 * g, 1)
        kv[c, core, yi, zi, RC:, :] = jnp.where(core == 0, packed[0:RP // 2], packed[RP // 2:]).astype(BF)
        return sc

    scale = HW ** -0.5 * math.log2(math.e)

    def queries(c, sc):
        rows = rows_of(c)
        q = dot(x_all[rows, :], w_q[...]) * (sc * scale)
        width = q.shape[1]
        if width % LANES:
            q = jnp.concatenate([q, jnp.zeros((RC, LANES - width % LANES), F32)], axis=1)
        qt = q.T
        blk, off = (chip + 1 + c // BC) % X, (c % BC) * RC
        cr, sr, cc, sn = [tab[i, :, rows] for i in range(4)]
        for h in range(H):
            low = (h % 2) * NOPE
            at = h * HW
            a, b, e, f = [qt[at + NOPE + 8 * i:at + NOPE + 8 * (i + 1)] for i in range(4)]
            qbuf[blk, h, low:low + NOPE, off:off + RC] = qt[at:at + NOPE].astype(BF)
            qbuf[blk, h, LANES:LANES + ROPE, off:off + RC] = jnp.concatenate(
                [a * cr - b * sr, b * cr + a * sr, e * cc - f * sn, f * cc + e * sn], axis=0).astype(BF)

    def conv_in(c, sc):
        rows = rows_of(c)
        xr = x_all[rows, :]
        inner = (dot(xr, w_conv[0]) * sc).astype(BF).astype(F32)
        value = (dot(xr, w_conv[1]) * sc).astype(BF).astype(F32)
        cprod[rows, :] = (inner * value).astype(BF)
        outer = (dot(xr, w_conv[2]) * sc).astype(BF).astype(F32)
        gate = (dot(xr, w_conv[3]) * sc).astype(BF).astype(F32)
        cgo[rows, :] = silu(gate) * outer

    def gate_in(c, sc):
        rows = rows_of(c)
        gat[rows, :] = silu((dot(x_all[rows, :], w_g[...]) * sc).astype(BF).astype(F32))

    def send_halo(k):
        src = cprod.at[pl.ds(R - EDGE, EDGE)] if k == 0 else cprod.at[pl.ds(0, EDGE)]
        to = (sp + 1) % n_sp if k == 0 else (sp + n_sp - 1) % n_sp
        return pltpu.make_async_remote_copy(
            src_ref=src, dst_ref=halo.at[k], send_sem=hsend.at[k], recv_sem=hrecv.at[k],
            device_id={"sp": to}, device_id_type=MESH)

    def build(c, t):
        kv_done(c, t)
        y = flip(yi, t)
        n = max(1, min(KB // RC, Z))
        for g0 in range(0, Z, n):
            k0 = pl.multiple_of((c * Y + y) * (Z * RC) + g0 * RC, n * RC)
            lats, ropes = [], []
            for z in range(g0, g0 + n):
                lats.append(jnp.concatenate([kv[c, 0, y, z, 0:RC, :], kv[c, 1, y, z, 0:RC, :]], axis=1))
                pk = jnp.concatenate([kv[c, 0, y, z, RC:, :], kv[c, 1, y, z, RC:, :]], axis=0).astype(F32)
                ropes += [pk if g == 0 else pltpu.roll(pk, LANES - 32 * g, 1) for g in range(4)]
            lat = jnp.concatenate(lats, axis=0)
            rows = pl.ds(k0, n * RC)
            kr[rows, :] = jnp.concatenate(ropes, axis=0).astype(BF)
            kn[rows, :] = dot(lat, w_k[...]).astype(BF)
            v = dot_t(v_t[...], lat).astype(BF)
            for h in range(H):
                vt[h, 0:VDIM, rows] = v[h * VDIM:(h + 1) * VDIM]

    def attend(kq, blocks):
        units = [(h, k0 + j * KB) for k0, count in blocks for j in range(count // KB) for h in range(H)]
        n = len(units)

        def score(u):
            h, k0 = units[u]
            rows = pl.ds(pl.multiple_of(k0, KB), KB)
            p = (h // 2) * LANES
            k = jnp.concatenate([kn[rows, p:p + LANES], kr[rows, :]], axis=1)
            sbuf[u % 3] = dot(k, qbuf[kq, h])

        def top(u):
            h, _ = units[u]
            old = mbuf[kq, h]
            new = jnp.maximum(old, jnp.max(sbuf[u % 3], axis=0, keepdims=True))
            mbuf[kq, h] = new
            return new, jnp.exp2(old - new)

        def weigh(u, p, shrink):
            h, k0 = units[u]
            acc[kq, h] = acc[kq, h] * shrink + dot(vt[h, :, pl.ds(pl.multiple_of(k0, KB), KB)], p)

        score(0)
        if n > 1:
            score(1)
        tops = {0: top(0)}
        last = None
        for u in range(n):
            if u + 2 < n:
                score(u + 2)
            if last is not None:
                weigh(*last)
            if u + 1 < n:
                tops[u + 1] = top(u + 1)
            new, shrink = tops.pop(u)
            last = (u, jnp.exp2(sbuf[u % 3] - new).astype(BF), shrink)
        weigh(*last)

    def line(c, t):
        return ((c * Y + flip(yi, t)) * (Z * RC), Z * RC)

    def chunks(kq, a, b):
        attend(kq, [(c * KC, KC) for c in range(a, b)])

    cross = list(range(1, Y))

    def take(c, peers):
        for t in peers:
            build(c, t)

    def heed(kq, c, peers):
        if peers:
            attend(kq, [line(c, t) for t in peers])

    def finish(kq):
        rows = pl.ds(pl.multiple_of(kq * RG, RG), RG)
        heads = []
        for h in range(H):
            a = acc[kq, h]
            heads.append(a[0:VDIM] / a[VDIM:VDIM + 1])
        attended = jnp.concatenate(heads, axis=0).T
        mix[rows, C:] = (gat[rows, :] * attended).astype(BF)

    def send_mate(d, i):
        return pltpu.make_async_remote_copy(
            src_ref=send_b.at[d, i], dst_ref=pbuf.at[d, i], send_sem=dsend.at[d], recv_sem=drecv.at[d, i],
            device_id={"tp": mate}, device_id_type=MESH)

    def send_x(d, i):
        return pltpu.make_async_remote_copy(
            src_ref=xbuf.at[d, i], dst_ref=rbuf.at[d, i], send_sem=xsend.at[d], recv_sem=xrecv.at[d, i],
            device_id={"tp": ((chip + d) % X) * 2 + core}, device_id_type=MESH)

    def block(kq, which, i):
        rows = pl.ds(pl.multiple_of(kq * RG + which * TB, TB), TB)
        return dot(mix[rows, :], w_down[:, i * DP:(i + 1) * DP]).astype(BF)

    def pair_sum(d, i):
        send_mate(d, i).wait_recv()
        return ybuf[i].astype(F32) + pbuf[d, i].astype(F32)

    def give(i):
        return pltpu.make_async_copy(obuf.at[i], out.at[:, i * DP:(i + 1) * DP], osem.at[i])

    def project_out(d):
        kq = (chip + d) % X

        def push(i):
            xbuf[d, i] = pair_sum(d, i).astype(BF)
            send_x(d, i).start()

        for i in range(NP):
            send_b[d, i] = block(kq, 1 - core, i)
            send_mate(d, i).start()
        for i in range(NP):
            ybuf[i] = block(kq, core, i)
            if d:
                push(i)

    def conv_out():
        send_halo(0).wait_recv()
        send_halo(1).wait_recv()
        cp = cprod[...].astype(F32)
        rid = lax.broadcasted_iota(jnp.int32, (R, C), 0)
        before = halo[0].astype(F32)[EDGE - 1:EDGE, :] * jnp.where(sp == 0, 0.0, 1.0)
        after = halo[1].astype(F32)[0:1, :] * jnp.where(sp == n_sp - 1, 0.0, 1.0)
        up = jnp.where(rid == 0, before, pltpu.roll(cp, 1, 0))
        down = jnp.where(rid == R - 1, after, pltpu.roll(cp, R - 1, 0))
        tw = taps[...].astype(F32)
        mix[:, 0:C] = (cgo[...] * (up * tw[0:1] + cp * tw[1:2] + down * tw[2:3])).astype(BF)

    near = [s for s in range(1, Z) if s < 2]
    far = [s for s in range(1, Z) if s >= 2]

    loads[0].wait()
    loads[1].wait()
    every = pl.ds(0, R)
    parts = [feature_part(every, tp)]
    for c in range(NC):
        send_tok(0, c).wait_recv()
    parts.append(feature_part(every, mate))
    zp[...], rpp[...], ssq[...] = add_parts(parts)

    lane = lax.broadcasted_iota(jnp.int32, (R, LANES), 1)
    pos = sp * R + lax.broadcasted_iota(jnp.int32, (R, LANES), 0)
    grid = jnp.where(lane < ROPE // 2, pos // GRID_W, pos % GRID_W).astype(F32)
    ang = grid * jnp.exp((lane % 8).astype(F32) * (-math.log(rope_theta) / 8.0))
    active = lane < ROPE
    first = (lane % 16) < 8
    sin = jnp.sin(ang)
    cosb[...] = jnp.where(active, jnp.cos(ang), 0.0)
    sina[...] = jnp.where(active & first, -sin, 0.0)
    sinb[...] = jnp.where(active & (~first), sin, 0.0)
    post = sp * R + lax.broadcasted_iota(jnp.int32, (8, R), 1)
    freq = jnp.exp(lax.broadcasted_iota(jnp.int32, (8, R), 0).astype(F32) * (-math.log(rope_theta) / 8.0))
    rang = (post // GRID_W).astype(F32) * freq
    cang = (post % GRID_W).astype(F32) * freq
    tab[0] = jnp.cos(rang)
    tab[1] = jnp.sin(rang)
    tab[2] = jnp.cos(cang)
    tab[3] = jnp.sin(cang)

    qbuf[...] = jnp.zeros(qbuf.shape, BF)
    ones = jnp.where(lax.broadcasted_iota(jnp.int32, (VROWS - VDIM, n_sp * R), 0) == 0, 1.0, 0.0).astype(BF)
    for h in range(H):
        vt[h, VDIM:VROWS, :] = ones
    mbuf[...] = jnp.full(mbuf.shape, -jnp.inf, F32)
    acc[...] = jnp.zeros(acc.shape, F32)


    scales = []
    for c in range(NC):
        rows = rows_of(c)
        parts = []
        for d in range(1, X):
            send_tok(d, c).wait_recv()
            relay_tok(d, c).start()
            parts.append(feature_part(rows, ((chip - d + X) % X) * 2 + core))
        if c == 1:
            for w in loads[2:]:
                w.wait()
            v_t[...] = w_v[...].astype(F32).T.astype(BF)
        if c:
            conv_in(c - 1, scales[c - 1])
        for d in range(1, X):
            relay_tok(d, c).wait_recv()
            parts.append(feature_part(rows, ((chip - d + X) % X) * 2 + 1 - core))
        scales.append(latents(c, parts))
        kv_start(c)
        if c and c - 1 < BC:
            queries(c - 1, scales[c - 1])
        if c >= 1:
            lines(c - 1, near)
        if c >= 2:
            lines(c - 2, far)
        if c and c - 1 < BC:
            gate_in(c - 1, scales[c - 1])
        if c == NC - 1:
            conv_in(c, scales[c])
            send_halo(0).start()
            send_halo(1).start()
        if c >= 1:
            crosses(c - 1, [0])
        if c >= 2:
            crosses(c - 2, near)
    first_q = (chip + 1) % X
    take(0, [0])
    heed(first_q, 0, [0])
    crosses(0, far)
    lines(2, far)
    lines(3, near)
    take(1, [0])
    take(0, cross)
    crosses(2, near)
    attend(first_q, [line(0, t) for t in cross] + [line(1, 0)])
    crosses(1, far)
    lines(3, far)
    take(2, [0])
    crosses(3, [0])
    take(1, cross)
    crosses(2, far)
    attend(first_q, [line(1, t) for t in cross] + [line(2, 0)])
    crosses(3, near)
    take(3, [0])
    crosses(3, far)
    take(2, cross)
    attend(first_q, [line(2, t) for t in cross] + [line(3, 0)])
    conv_out()
    take(3, cross)
    heed(first_q, 3, cross)
    finish(first_q)
    for d in range(1, X):
        project_out(d)
        kq = (chip + d + 1) % X
        if d == 1:
            for c in range(BC, NC):
                queries(c, scales[c])
                gate_in(c, scales[c])
        for c in range(NC):
            chunks(kq, c, c + 1)
        finish(kq)
    project_out(0)

    for i in range(NP):
        total = pair_sum(0, i)
        for d in range(1, X):
            send_x(d, i).wait_recv()
            total = total + rbuf[d, i].astype(F32)
        obuf[i] = total.astype(BF)
        give(i).start()

    def sent(ref, sem):
        pltpu.make_async_copy(ref, ref, sem).wait()

    for d in range(X):
        sent(x_all.at[:, cols(tp)], tsend.at[d])
        sent(send_b.at[d], dsend.at[d])
        if d:
            sent(x_all.at[:, cols(tp)], rsend.at[d])
            sent(xbuf.at[d], xsend.at[d])
    sent(kv.at[:, core, 0, pl.ds(0, Z - 1)], zsend.at[0])
    sent(kv.at[:, core, pl.ds(0, Y - 1)], ysend.at[0])
    sent(kv.at[:, core], msend.at[0])
    send_halo(0).wait_send()
    send_halo(1).wait_send()
    for i in range(NP):
        give(i).wait()
def on_device(n_sp, n_tp, tokens, wci, wcn, wco, wcg, taps, wq, wl, wr, gain, ku, vu, wg, cd, ad):
    R, fl = tokens.shape
    D, C = wci.shape
    KV = wl.shape[1]
    H = ku.shape[1] // NOPE
    A = H * VDIM
    X = n_tp // 2
    Y = X if n_sp % X == 0 else 1
    Z = n_sp // Y
    RG, TB = R // X, R // n_tp
    NC, NP = 4, 4
    RC = R // NC
    DP = D // NP
    S = n_sp * R
    KB = min(512, n_sp * RC)
    dma = pltpu.SemaphoreType.DMA
    anys = pl.BlockSpec(memory_space=pl.ANY)
    vm = pl.BlockSpec(memory_space=pltpu.VMEM)
    V = pltpu.VMEM
    return pl.pallas_call(
        functools.partial(body, (n_sp, n_tp, Y, Z, R, fl, D, H, C, KV, NC, NP, KB)),
        out_shape=jax.ShapeDtypeStruct((TB, cd.shape[1]), BF),
        in_specs=[anys] * 13 + [vm] * 2,
        out_specs=anys,
        scratch_shapes=[
            V((R, D), BF), V((4, D, C), BF), V(wq.shape, BF), V((D, A), BF),
            V((D, KV), BF), V((ROPE, D), BF), V(ku.shape, BF), V(vu.shape, BF),
            V((A, KV), BF), V((C + A, cd.shape[1]), BF),
            V((NC, 2, Y, Z, RC + RC // 8, LANES), BF),
            V((S, H * NOPE), BF), V((S, LANES), BF), V((H, VROWS, S), BF), V((X, H, 2 * LANES, RG), BF),
            V((R, LANES), F32), V((R, LANES), F32), V((R, LANES), F32), V((4, 8, R), F32),
            V((R, C), BF), V((R, C), F32), V((R, A), F32), V((2, EDGE, C), BF), V((R, C + A), BF),
            V((X, H, 1, RG), F32), V((X, H, VROWS, RG), F32), V((3, KB, RG), F32),
            V((X, NP, TB, DP), BF), V((X, NP, TB, DP), BF),
            V((X, NP, TB, DP), BF), V((X, NP, TB, DP), BF), V((NP, TB, DP), BF), V((NP, TB, DP), BF),
            V((R, KV), F32), V((R, ROPE), F32), V((R, 1), F32),
            dma((13,)), dma((X,)), dma((X, NC)), dma((X,)), dma((X, NC)),
            dma((1,)), dma((NC, Z)), dma((1,)), dma((NC, Y, Z)), dma((1,)), dma((NC, Y)),
            dma((2,)), dma((2,)),
            dma((X,)), dma((X, NP)), dma((X,)), dma((X, NP)), dma((NP,)),
        ],
        compiler_params=pltpu.CompilerParams(
            collective_id=0, has_side_effects=True, vmem_limit_bytes=60 * 1024 * 1024),
    )(tokens, wci, wcn, wco, wcg, wq, wg, wl, wr.T, cd, ad, ku, vu, taps, gain.reshape(1, KV))


def solution(mesh):
    tp = P(None, "tp")
    placed = (P("sp", "tp"), tp, tp, tp, tp, tp, tp, P(), P(), P(), tp, tp, tp,
              P("tp", None), P("tp", None))
    return jax.shard_map(
        functools.partial(on_device, mesh.shape["sp"], mesh.shape["tp"]),
        mesh=mesh, in_specs=placed, out_specs=P(("sp", "tp"), None), check_vma=False)
```
